512 devices in a mesh: sp: 16 (over z), fs: 4 (over y), tp: 8 (over x, core).
Axes of the slice: x: 4, y: 4, z: 16, core: 2. Of those that a mesh axis runs over, the one named last changes fastest.
Arguments:
- inputs: bfloat16 [4, 8192, 2048], P('fs', 'sp', 'tp'), may hold values from -6 to 6
- norm_gain: float32 [2048], replicated, may hold values from 0.1 to 1.9
- query_weight: bfloat16 [2048, 1024], P(('sp', 'fs'), 'tp'), may hold values from -0.125 to 0.125
- key_weight: bfloat16 [2048, 1024], P(('sp', 'fs'), 'tp'), may hold values from -0.125 to 0.125
- value_weight: bfloat16 [2048, 1024], P(('sp', 'fs'), 'tp'), may hold values from -0.125 to 0.125
- query_gain: float32 [64], replicated, may hold values from 0.8 to 7
- key_gain: float32 [64], replicated, may hold values from 0.8 to 7
- mix_lambda: float32 [8], replicated, may hold values from 0.3 to 0.8
- head_gain: float32 [128], replicated, may hold values from 0.1 to 1.9
- post_gate_weight: bfloat16 [2048, 2048], P(('sp', 'fs'), 'tp'), may hold values from -0.125 to 0.125
- pre_gate_weight: bfloat16 [2048, 2048], P(('sp', 'fs'), 'tp'), may hold values from -0.125 to 0.125
- inner_weight: bfloat16 [2048, 2048], P(('sp', 'fs'), 'tp'), may hold values from -0.125 to 0.125
- conv_taps: float32 [3, 2048], replicated, may hold values from -3 to 3
- attn_out_weight: bfloat16 [2048, 1024], P(('sp', 'fs'), 'tp'), may hold values from -0.109375 to 0.109375
- conv_out_weight: bfloat16 [2048, 2048], P(('sp', 'fs'), 'tp'), may hold values from -0.109375 to 0.109375
Outputs:
- mixed: bfloat16 [4, 8192, 2048], P('fs', ('sp', 'tp'))
The draws below stay inside these ranges and needn't reach their ends.
All inputs are finite; a program needn't handle non-finite values.
Results may differ from the reference program's by a relative error of at most 0.015.
The reference program's roundings to bfloat16 on the way count: a program that leaves them out, or rounds other values in their place, can miss the bound.
Values may be sent and summed in bfloat16 or wider, within the bound.
A program may use at most 64 MiB of HBM per device.

```python
import math
import jax
import jax.numpy as jnp
from jax import lax

D = 2048
HEADS = 8
HALF = 64
VDIM = 128
LENGTH = 8192
SEQS = 4
N_TP = 8


def gain_draw(key, salt):
    lowest = 0.8
    highest = 1.8
    fraction = jax.random.uniform(jax.random.fold_in(key, salt), (HALF,), jnp.float32)
    return jnp.exp(jnp.log(lowest) + fraction * (jnp.log(highest) - jnp.log(lowest)))


def draw_query_gain(key, part):
    return gain_draw(key, 31)


def draw_key_gain(key, part):
    return gain_draw(key, 57)


def steps_of(own_key, shape, pieces, least, largest):
    level, own = 1.0, jax.random.fold_in(own_key, 6)
    for dim, parts in pieces:
        draws = jnp.exp(jax.random.uniform(jax.random.fold_in(own, dim), (parts,), jnp.float32, least / len(pieces), largest / len(pieces)))
        level = level * jnp.repeat(draws, shape[dim] // parts).reshape([-1 if axis == dim else 1 for axis in range(len(shape))])
    return level


def centred(rng, extent, scale, most, cuts=(), kind=jnp.bfloat16):
    values = jax.random.normal(rng, extent, jnp.float32) * scale
    if len(cuts) > 0:
        values = steps_of(rng, extent, cuts, -0.22, 0.18) * values
    return jnp.clip(values, min=-most, max=most).astype(kind)


def setup_inputs(seed: int = 0) -> dict:
    keys = jax.random.split(jax.random.key(seed), 16)
    return {
        "inputs": centred(keys[0], (SEQS, LENGTH, D), 1.0, 6.0, ((0, 4), (1, 16), (2, 8))),
        "norm_gain": jnp.clip(1.0 + 0.18 * jax.random.normal(keys[1], (D,), jnp.float32), 0.1, 1.9),
        "query_weight": centred(keys[2], (D, HEADS * 2 * HALF), D ** -0.5, 0.125, ((0, 64), (1, 8))),
        "key_weight": centred(keys[3], (D, HEADS * 2 * HALF), D ** -0.5, 0.125, ((0, 64), (1, 8))),
        "value_weight": centred(keys[4], (D, HEADS * VDIM), D ** -0.5, 0.125, ((0, 64), (1, 8))),
        "query_gain": draw_query_gain(jax.random.fold_in(keys[15], 71), 0),
        "key_gain": draw_key_gain(jax.random.fold_in(keys[15], 71), 0),
        "mix_lambda": jnp.clip(jax.random.uniform(keys[7], (HEADS,), jnp.float32, 0.3, 0.8), 0.3, 0.8),
        "head_gain": jnp.clip(1.0 + 0.18 * jax.random.normal(keys[8], (VDIM,), jnp.float32), 0.1, 1.9),
        "post_gate_weight": centred(keys[9], (D, D), D ** -0.5, 0.125, ((0, 64), (1, 8))),
        "pre_gate_weight": centred(keys[10], (D, D), D ** -0.5, 0.125, ((0, 64), (1, 8))),
        "inner_weight": centred(keys[11], (D, D), D ** -0.5, 0.125, ((0, 64), (1, 8))),
        "conv_taps": centred(keys[12], (3, D), 0.6, 3.0, (), jnp.float32),
        "attn_out_weight": centred(keys[13], (D, HEADS * VDIM), (HEADS * VDIM + D) ** -0.5, 0.109375, ((0, 64), (1, 8))),
        "conv_out_weight": centred(keys[14], (D, D), (HEADS * VDIM + D) ** -0.5, 0.109375, ((0, 64), (1, 8))),
    }


epsilon = 1e-06

def scale_rows(values, gain):
    return values * lax.rsqrt(lax.optimization_barrier(jnp.mean(values * values, axis=-1, keepdims=True)) + epsilon) * gain

def attend_head(query_head, key_head, value_head, weight_two):
    block = math.gcd(LENGTH, 512)
    query_blocks = jnp.transpose(query_head.reshape(2, LENGTH // block, block, HALF), (1, 0, 2, 3))
    keys_wide = key_head.astype(jnp.float32)
    values_wide = value_head.astype(jnp.float32)

    def one_block(query_block):
        scores = jnp.einsum('jqd,jkd->jqk', query_block.astype(jnp.float32), keys_wide) * HALF ** (-0.5)
        peak = lax.optimization_barrier(jnp.max(scores, axis=-1, keepdims=True))
        expo = jnp.exp(scores - peak)
        total = lax.optimization_barrier(jnp.sum(expo, axis=-1, keepdims=True))
        rounded = lax.optimization_barrier(expo.astype(jnp.bfloat16)).astype(jnp.float32)
        mapped = jnp.einsum('jqk,kd->jqd', rounded, values_wide) / total
        return mapped[0] - weight_two * mapped[1]
    result = lax.map(one_block, query_blocks)
    return result.reshape(LENGTH, VDIM)

def one_sequence(tokens, norm_gain, query_weight, key_weight, value_weight, query_gain, key_gain, mix_lambda, head_gain, post_gate_weight, pre_gate_weight, inner_weight, conv_taps, attn_out_weight, conv_out_weight):
    normed = scale_rows(tokens.astype(jnp.float32), norm_gain).astype(jnp.bfloat16)
    query = jnp.dot(normed, query_weight, preferred_element_type=jnp.float32).reshape(LENGTH, HEADS, 2, HALF)
    key = jnp.dot(normed, key_weight, preferred_element_type=jnp.float32).reshape(LENGTH, HEADS, 2, HALF)
    query_normed = scale_rows(query, query_gain).astype(jnp.bfloat16)
    key_normed = scale_rows(key, key_gain).astype(jnp.bfloat16)
    values = jnp.dot(normed, value_weight, preferred_element_type=jnp.float32).astype(jnp.bfloat16)
    values = values.reshape(LENGTH, HEADS, VDIM)

    def per_head(members):
        return attend_head(members[0], members[1], members[2], members[3])
    head_out = lax.map(per_head, (jnp.transpose(query_normed, (1, 2, 0, 3)), jnp.transpose(key_normed, (1, 2, 0, 3)), jnp.transpose(values, (1, 0, 2)), mix_lambda))
    attn_hidden = scale_rows(head_out, head_gain).astype(jnp.bfloat16)
    attn_hidden = jnp.transpose(attn_hidden, (1, 0, 2)).reshape(LENGTH, HEADS * VDIM)
    post = jnp.dot(normed, post_gate_weight, preferred_element_type=jnp.float32).astype(jnp.bfloat16)
    post_wide = lax.optimization_barrier(post).astype(jnp.float32)
    signal = (jnp.dot(normed, pre_gate_weight, preferred_element_type=jnp.float32) * jnp.dot(normed, inner_weight, preferred_element_type=jnp.float32)).astype(jnp.bfloat16)
    padded = jnp.pad(lax.optimization_barrier(signal).astype(jnp.float32), ((1, 1), (0, 0)))
    filtered = conv_taps[0] * padded[:-2] + conv_taps[1] * padded[1:-1] + conv_taps[2] * padded[2:]
    conv_hidden = (post_wide * filtered).astype(jnp.bfloat16)
    head_span = HEADS // N_TP * VDIM
    channel_span = D // N_TP
    summed = jnp.zeros((LENGTH, D), jnp.float32)
    for group in range(N_TP):
        attn_part = attn_hidden[:, group * head_span:(group + 1) * head_span]
        attn_cols = attn_out_weight[:, group * head_span:(group + 1) * head_span]
        conv_part = conv_hidden[:, group * channel_span:(group + 1) * channel_span]
        conv_cols = conv_out_weight[:, group * channel_span:(group + 1) * channel_span]
        partial_value = jnp.dot(attn_part, attn_cols.T, preferred_element_type=jnp.float32) + jnp.dot(conv_part, conv_cols.T, preferred_element_type=jnp.float32)
        summed = summed + lax.optimization_barrier(partial_value.astype(jnp.bfloat16)).astype(jnp.float32)
    return summed.astype(jnp.bfloat16)

def reference(inputs, norm_gain, query_weight, key_weight, value_weight, query_gain, key_gain, mix_lambda, head_gain, post_gate_weight, pre_gate_weight, inner_weight, conv_taps, attn_out_weight, conv_out_weight):
    results = []
    for sequence in range(SEQS):
        results.append(one_sequence(inputs[sequence], norm_gain, query_weight, key_weight, value_weight, query_gain, key_gain, mix_lambda, head_gain, post_gate_weight, pre_gate_weight, inner_weight, conv_taps, attn_out_weight, conv_out_weight))
    return jnp.stack(results, axis=0)
```

```python
import functools

import jax
import jax.numpy as jnp
from jax import lax
from jax.experimental import pallas as pl
from jax.experimental.pallas import tpu as pltpu
from jax.sharding import PartitionSpec as P

EPS = 1e-06
MESH = pl.DeviceIdType.MESH
F32 = jnp.float32
BF16 = jnp.bfloat16
LOG2E = 1.4426950408889634

NZ, NY, NX = 16, 4, 4
CH1, CH2 = 4, 2


def body(
    tok_ref, wq_ref, wk_ref, wv_ref, wpost_ref, wpre_ref, winner_ref, wao_ref, wco_ref,
    ngain_ref, qgain_ref, kgain_ref, hgain_ref, taps_ref, lam_ref,
    out_ref,
    xg, nrm, w0, w1, w2, kb, vb, qb, m_s, l_s, acc_s, hid, sigb, sigf, halo, postb,
    part, pair_in, psum, rel, fin,
    lsem, xss, xrs, zss, zrs, yds, ydr, yfs, yfr, y1ds, y1dr, y1fs, y1fr,
    y2ds, y2dr, y2fs, y2fr, kvs, kvr, hs, hr, rs, rr,
):
    z = lax.axis_index("sp")
    y = lax.axis_index("fs")
    t = lax.axis_index("tp")
    x = t // 2
    c = t % 2

    def zz(i):
        return (i + 2 * NZ) % NZ

    def yy(i):
        return (i + 2 * NY) % NY

    def xx(i):
        return (i + 2 * NX) % NX

    dev_z = ({"sp": zz(z + 1)}, {"sp": zz(z - 1)})
    dev_y = ({"fs": yy(y + 1)}, {"fs": yy(y - 1)})
    dev_x = ({"tp": xx(x + 1) * 2 + c}, {"tp": xx(x - 1) * 2 + c})
    other = x * 2 + (1 - c)
    dev_c = {"tp": other}
    peers = dev_z + dev_y + dev_x + (dev_c,)

    def rc(src, dst, ssem, rsem, dev):
        return pltpu.make_async_remote_copy(
            src_ref=src, dst_ref=dst, send_sem=ssem, recv_sem=rsem,
            device_id=dev, device_id_type=MESH,
        )

    own = (
        (tok_ref, xg.at[t]),
        (wq_ref, w0.at[z, y, :, 0:128]),
        (wk_ref, w0.at[z, y, :, 128:256]),
        (wv_ref, w0.at[z, y, :, 256:384]),
        (wpost_ref, w1.at[z, y, :, 0:256]),
        (wpre_ref, w1.at[z, y, :, 256:512]),
        (winner_ref, w1.at[z, y, :, 512:768]),
        (wao_ref, w2.at[z, y, :, 0:128]),
        (wco_ref, w2.at[z, y, :, 128:384]),
    )
    local = [pltpu.make_async_copy(s, d, lsem.at[i]) for i, (s, d) in enumerate(own)]
    for cp in local:
        cp.start()
    barrier = pltpu.get_barrier_semaphore()
    for dev in peers:
        pl.semaphore_signal(barrier, inc=1, device_id=dev, device_id_type=MESH)

    qb[...] = jnp.zeros_like(qb)
    m_s[...] = jnp.full_like(m_s, -1e30)
    l_s[...] = jnp.zeros_like(l_s)
    acc_s[...] = jnp.zeros_like(acc_s)

    pl.semaphore_wait(barrier, len(peers))

    pending = []

    def go(copy):
        copy.start()
        pending.append(copy)

    ws = (w0, w1, w2)
    zsteps = ((7, 8), (8, 7), (7, 8))

    def z_copy(g, d, s):
        i = zz(z - (s - 1)) if d == 0 else zz(z + (s - 1))
        w = ws[g]
        return rc(w.at[i, y], w.at[i, y], zss.at[g, d, s - 1], zrs.at[g, d, s - 1], dev_z[d])

    def z_wait(g, d, s):
        i = zz(z - s) if d == 0 else zz(z + s)
        w = ws[g]
        rc(w.at[i, y], w.at[i, y], zss.at[g, d, s - 1], zrs.at[g, d, s - 1], dev_z[d]).wait_recv()

    def y0_send(k, i):
        for d in range(2):
            go(rc(w0.at[i, y], w0.at[i, y], yds.at[d, k], ydr.at[d, k], dev_y[d]))

    def y0_forward(k, i):
        for d in range(2):
            col = yy(y - 1) if d == 0 else yy(y + 1)
            rc(w0.at[i, col], w0.at[i, col], yds.at[d, k], ydr.at[d, k], dev_y[d]).wait_recv()
            half = w0.at[i, col, pl.ds(16 * d, 16)]
            go(rc(half, half, yfs.at[d, k], yfr.at[d, k], dev_y[d]))

    def y0_finish(k, i):
        for d in range(2):
            col = yy(y + 2)
            half = w0.at[i, col, pl.ds(16 * d, 16)]
            rc(half, half, yfs.at[d, k], yfr.at[d, k], dev_y[d]).wait_recv()

    def x_send(k, slot, dev, rows=None):
        ref = xg.at[slot] if rows is None else xg.at[slot, rows]
        go(rc(ref, ref, xss.at[k], xrs.at[k], dev))

    def x_wait(k, slot, rows=None):
        ref = xg.at[slot] if rows is None else xg.at[slot, rows]
        rc(ref, ref, xss.at[k], xrs.at[k], dev_c).wait_recv()

    lo, hi = pl.ds(0, 256), pl.ds(256, 256)
    left, right, far = xx(x - 1), xx(x + 1), xx(x + 2)

    local[1].wait()
    local[2].wait()
    local[3].wait()
    for d in range(2):
        go(z_copy(0, d, 1))
    local[0].wait()
    x_send(0, t, dev_x[0])
    x_send(1, t, dev_x[1])
    x_send(2, t, dev_c)
    y0_send(0, z)
    for i in range(4, 9):
        local[i].wait()
    for g in (1, 2):
        for d in range(2):
            go(z_copy(g, d, 1))

    def slabs_of(s):
        result = []
        if zsteps[0][0] >= s:
            result.append((2 * s - 1, zz(z - s)))
        if zsteps[0][1] >= s:
            result.append((2 * s if zsteps[0][0] >= s else 2 * s - 1, zz(z + s)))
        return result

    def x_service_a():
        x_wait(0, left * 2 + c)
        x_send(5, left * 2 + c, dev_x[0], lo)
        x_wait(1, right * 2 + c)
        x_send(6, right * 2 + c, dev_x[1], hi)
        x_send(3, left * 2 + c, dev_c)
        x_send(4, right * 2 + c, dev_c)

    def x_service_b():
        x_wait(5, far * 2 + c, lo)
        x_send(7, far * 2 + c, dev_c, lo)
        x_wait(6, far * 2 + c, hi)
        x_send(8, far * 2 + c, dev_c, hi)

    def x_finish():
        x_wait(2, other)
        x_wait(3, left * 2 + (1 - c))
        x_wait(4, right * 2 + (1 - c))
        x_wait(7, far * 2 + (1 - c), lo)
        x_wait(8, far * 2 + (1 - c), hi)

    def normalize():
        def tile(i, carry):
            rows = pl.ds(pl.multiple_of(i * 32, 32), 32)
            total = jnp.zeros((32, 256), F32)
            for b in range(8):
                v = xg[b, rows, :].astype(F32)
                total = total + v * v
            r = lax.rsqrt(jnp.sum(total, axis=-1, keepdims=True) * (1.0 / 2048) + EPS)
            for b in range(8):
                v = xg[b, rows, :].astype(F32) * r * ngain_ref[:, b * 256 : (b + 1) * 256]
                nrm[rows, b * 256 : (b + 1) * 256] = v.astype(BF16)
            return carry

        lax.fori_loop(0, 16, tile, 0)

    for s in range(1, 9):
        for g in range(3):
            for d in range(2):
                if zsteps[g][d] >= s:
                    z_wait(g, d, s)
                    if zsteps[g][d] > s:
                        go(z_copy(g, d, s + 1))
            if g == 0:
                for k, i in slabs_of(s):
                    y0_send(k, i)
                if s == 2:
                    y0_forward(0, z)
                if s >= 3:
                    for k, i in slabs_of(s - 2):
                        y0_forward(k, i)
        if s == 3:
            x_service_a()
        if s == 5:
            x_service_b()
        if s == 6:
            x_finish()
            normalize()
    for s in (7, 8):
        for k, i in slabs_of(s):
            y0_forward(k, i)

    def yc(w, n, d, k, col, forward):
        span = NZ // n
        if forward:
            return w.at[pl.ds(k * span + d * (span // 2), span // 2), col]
        return w.at[pl.ds(k * span, span), col]

    y_sets = {1: (w1, CH1, y1ds, y1dr, y1fs, y1fr), 2: (w2, CH2, y2ds, y2dr, y2fs, y2fr)}

    def y_direct(g, k, d):
        w, n, ds, dr, _, _ = y_sets[g]
        ref = yc(w, n, d, k, y, False)
        return rc(ref, ref, ds.at[d, k], dr.at[d, k], dev_y[d])

    def y_forward(g, k, d):
        w, n, _, _, fs, fr = y_sets[g]
        ref = yc(w, n, d, k, yy(y - 1) if d == 0 else yy(y + 1), True)
        return rc(ref, ref, fs.at[d, k], fr.at[d, k], dev_y[d])

    def y_direct_wait(g, k, d):
        w, n, ds, dr, _, _ = y_sets[g]
        ref = yc(w, n, d, k, yy(y - 1) if d == 0 else yy(y + 1), False)
        rc(ref, ref, ds.at[d, k], dr.at[d, k], dev_y[d]).wait_recv()

    def y_forward_wait(g, k, d):
        w, n, _, _, fs, fr = y_sets[g]
        ref = yc(w, n, d, k, yy(y + 2), True)
        rc(ref, ref, fs.at[d, k], fr.at[d, k], dev_y[d]).wait_recv()

    for k in range(CH1):
        for d in range(2):
            go(y_direct(1, k, d))

    y0_finish(0, z)
    for s in range(1, 9):
        for k, i in slabs_of(s):
            y0_finish(k, i)

    lane = lax.broadcasted_iota(jnp.int32, (128, 128), 1)
    first = lane < 64

    def half_norm(v, gain):
        sq = v * v
        s1 = jnp.sum(jnp.where(first, sq, 0.0), axis=-1, keepdims=True)
        s2 = jnp.sum(jnp.where(first, 0.0, sq), axis=-1, keepdims=True)
        r = jnp.where(
            first, lax.rsqrt(s1 * (1.0 / 64) + EPS), lax.rsqrt(s2 * (1.0 / 64) + EPS)
        )
        return v * r * gain

    def qkv_tile(i, carry):
        rows = pl.ds(pl.multiple_of(i * 128, 128), 128)
        rows2 = pl.ds(pl.multiple_of(i * 128 + 512, 128), 128)
        qkv = jnp.dot(
            nrm[rows, :], w0[...].reshape(2048, 384), preferred_element_type=F32
        )
        kb[z, rows, :] = half_norm(qkv[:, 128:256], kgain_ref[...]).astype(BF16)
        vb[z, :, rows] = qkv[:, 256:384].T.astype(BF16)
        qt = half_norm(qkv[:, 0:128], qgain_ref[...]).T.astype(BF16)
        qb[0:64, rows] = qt[0:64]
        qb[64:128, rows2] = qt[64:128]
        return carry

    lax.fori_loop(0, 4, qkv_tile, 0)

    bufs = (kb, vb)

    def kv_copy(d, w, s):
        i = zz(z - (s - 1)) if d == 0 else zz(z + (s - 1))
        ref = bufs[w].at[i]
        return rc(ref, ref, kvs.at[d, w, s - 1], kvr.at[d, w, s - 1], dev_z[d])

    def kv_wait(d, w, s):
        i = zz(z - s) if d == 0 else zz(z + s)
        ref = bufs[w].at[i]
        rc(ref, ref, kvs.at[d, w, s - 1], kvr.at[d, w, s - 1], dev_z[d]).wait_recv()

    for w in range(2):
        for d in range(2):
            kv_copy(d, w, 1).start()

    factor = LOG2E * 0.125

    def attend(b):
        def tile(j, carry):
            cols = pl.ds(pl.multiple_of(j * 256, 256), 256)
            st = jnp.dot(kb[b], qb[:, cols], preferred_element_type=F32)
            m_old = m_s[:, cols]
            m_new = jnp.maximum(m_old, jnp.max(st, axis=0, keepdims=True))
            p = jnp.exp2((st - m_new) * factor)
            a = jnp.exp2((m_old - m_new) * factor)
            l_s[:, cols] = l_s[:, cols] * a + jnp.sum(p, axis=0, keepdims=True)
            acc_s[:, cols] = acc_s[:, cols] * a + jnp.dot(
                vb[b], p.astype(BF16), preferred_element_type=F32
            )
            m_s[:, cols] = m_new
            return carry

        lax.fori_loop(0, 4, tile, 0)

    attend(z)

    def conv_project():
        def tile(i, carry):
            rows = pl.ds(pl.multiple_of(i * 128, 128), 128)
            rows8 = pl.ds(pl.multiple_of(i * 128 + 8, 8), 128)
            r = jnp.dot(nrm[rows, :], w1[...].reshape(2048, 768), preferred_element_type=F32)
            postb[rows, :] = r[:, 0:256].astype(BF16)
            signal = (r[:, 256:512] * r[:, 512:768]).astype(BF16)
            sigb[rows, :] = signal
            sigf[rows8, :] = signal.astype(F32)
            return carry

        lax.fori_loop(0, 4, tile, 0)

    def halo_copy(d):
        src = sigb.at[pl.ds(496, 16)] if d == 0 else sigb.at[pl.ds(0, 16)]
        return rc(src, halo.at[d], hs.at[d], hr.at[d], dev_z[d])

    def conv_filter():
        before = halo[0].astype(F32)[8:16]
        after = halo[1].astype(F32)[0:8]
        sigf[0:8, :] = jnp.where(z > 0, before, 0.0)
        sigf[520:528, :] = jnp.where(z < NZ - 1, after, 0.0)
        taps = taps_ref[:, pl.ds(pl.multiple_of(t * 256, 256), 256)]
        for i in range(4):
            r = i * 128
            filtered = (
                taps[0:1] * sigf[r + 7 : r + 135, :]
                + taps[1:2] * sigf[r + 8 : r + 136, :]
                + taps[2:3] * sigf[r + 9 : r + 137, :]
            )
            hid[r : r + 128, 128:384] = (
                postb[r : r + 128, :].astype(F32) * filtered
            ).astype(BF16)

    def kv_step(s, carry):
        for w in range(2):
            for d in range(2):
                kv_wait(d, w, s)
                if d == w:
                    kv_copy(d, w, s + 1).start()
                else:

                    @pl.when(s < 7)
                    def _():
                        kv_copy(d, w, s + 1).start()

        for k in range(CH1):

            @pl.when(s == k + 1)
            def _():
                for d in range(2):
                    y_direct_wait(1, k, d)
                    y_forward(1, k, d).start()

        for k in range(CH2):

            @pl.when(s == k + 3)
            def _():
                for d in range(2):
                    y_direct(2, k, d).start()

            @pl.when(s == k + 6)
            def _():
                for d in range(2):
                    y_direct_wait(2, k, d)
                    y_forward(2, k, d).start()

        attend(zz(z - s))
        attend(zz(z + s))

        @pl.when(s == 6)
        def _():
            for k in range(CH1):
                for d in range(2):
                    y_forward_wait(1, k, d)
            conv_project()
            for d in range(2):
                halo_copy(d).start()

        @pl.when(s == 7)
        def _():
            for d in range(2):
                halo_copy(d).wait_recv()
            conv_filter()

        return carry

    lax.fori_loop(1, 8, kv_step, 0)
    for k in range(CH2):
        for d in range(2):
            y_forward_wait(2, k, d)
    kv_wait(0, 0, 8)
    kv_wait(1, 1, 8)
    attend(zz(z + 8))

    lam = lam_ref[t]
    inv = 1.0 / l_s[...]
    head = acc_s[:, 0:512] * inv[:, 0:512] - lam * (acc_s[:, 512:1024] * inv[:, 512:1024])
    r = lax.rsqrt(jnp.sum(head * head, axis=0, keepdims=True) * (1.0 / 128) + EPS)
    hid[:, 0:128] = ((head * r).T * hgain_ref[...]).astype(BF16)

    def out_tile(n, carry):
        cols = pl.ds(pl.multiple_of(n * 256, 256), 256)
        w = w2[pl.ds(n * 2, 2)].reshape(256, 384)
        r = lax.dot_general(
            hid[...], w, (((1,), (1,)), ((), ())), preferred_element_type=F32
        )
        part[:, :, :, cols] = r.astype(BF16).reshape(NX, 2, 64, 256)
        return carry

    lax.fori_loop(0, 8, out_tile, 0)

    pair = rc(part.at[:, 1 - c], pair_in, rs.at[0], rr.at[0], dev_c)
    pair.start()
    pair.wait_recv()
    up, down = pl.ds(0, 32), pl.ds(32, 32)

    def sum_pair(j):
        psum[j] = (part[j, c].astype(F32) + pair_in[j].astype(F32)).astype(BF16)

    sum_pair(far)
    r1 = rc(psum.at[far, up], rel.at[0], rs.at[1], rr.at[1], dev_x[0])
    r1.start()
    r2 = rc(psum.at[far, down], rel.at[1], rs.at[2], rr.at[2], dev_x[1])
    r2.start()
    sum_pair(right)
    sum_pair(left)
    r3 = rc(psum.at[right, down], fin.at[0, down], rs.at[3], rr.at[3], dev_x[0])
    r3.start()
    r4 = rc(psum.at[left, up], fin.at[1, up], rs.at[4], rr.at[4], dev_x[1])
    r4.start()
    r1.wait_recv()
    psum[right, 0:32] = (psum[right, 0:32].astype(F32) + rel[0].astype(F32)).astype(BF16)
    r5 = rc(psum.at[right, up], fin.at[0, up], rs.at[5], rr.at[5], dev_x[0])
    r5.start()
    r2.wait_recv()
    psum[left, 32:64] = (psum[left, 32:64].astype(F32) + rel[1].astype(F32)).astype(BF16)
    r6 = rc(psum.at[left, down], fin.at[1, down], rs.at[6], rr.at[6], dev_x[1])
    r6.start()
    mine = part[x, c].astype(F32) + pair_in[x].astype(F32)
    for cp in (r3, r4, r5, r6):
        cp.wait_recv()
    out_ref[...] = (mine + fin[0].astype(F32) + fin[1].astype(F32)).astype(BF16)

    for cp in pending:
        cp.wait_send()
    for w in range(2):
        for d in range(2):
            for s in range(1, 9 if d == w else 8):
                kv_copy(d, w, s).wait_send()
    for g, n in ((1, CH1), (2, CH2)):
        for k in range(n):
            for d in range(2):
                if g == 2:
                    y_direct(g, k, d).wait_send()
                y_forward(g, k, d).wait_send()
    for d in range(2):
        halo_copy(d).wait_send()
    for cp in (pair, r1, r2, r3, r4, r5, r6):
        cp.wait_send()


def per_device(
    inputs, norm_gain, query_weight, key_weight, value_weight, query_gain, key_gain,
    mix_lambda, head_gain, post_gate_weight, pre_gate_weight, inner_weight, conv_taps,
    attn_out_weight, conv_out_weight,
):
    hbm = pl.BlockSpec(memory_space=pl.ANY)
    vmem = pl.BlockSpec(memory_space=pltpu.VMEM)
    smem = pl.BlockSpec(memory_space=pltpu.SMEM)
    sem = pltpu.SemaphoreType.DMA
    out = pl.pallas_call(
        body,
        out_shape=jax.ShapeDtypeStruct((64, 2048), BF16),
        in_specs=[hbm] * 9 + [vmem] * 5 + [smem],
        out_specs=vmem,
        scratch_shapes=[
            pltpu.VMEM((8, 512, 256), BF16),
            pltpu.VMEM((512, 2048), BF16),
            pltpu.VMEM((NZ, NY, 32, 384), BF16),
            pltpu.VMEM((NZ, NY, 32, 768), BF16),
            pltpu.VMEM((NZ, NY, 32, 384), BF16),
            pltpu.VMEM((NZ, 512, 128), BF16),
            pltpu.VMEM((NZ, 128, 512), BF16),
            pltpu.VMEM((128, 1024), BF16),
            pltpu.VMEM((1, 1024), F32),
            pltpu.VMEM((1, 1024), F32),
            pltpu.VMEM((128, 1024), F32),
            pltpu.VMEM((512, 384), BF16),
            pltpu.VMEM((512, 256), BF16),
            pltpu.VMEM((528, 256), F32),
            pltpu.VMEM((2, 16, 256), BF16),
            pltpu.VMEM((512, 256), BF16),
            pltpu.VMEM((NX, 2, 64, 2048), BF16),
            pltpu.VMEM((NX, 64, 2048), BF16),
            pltpu.VMEM((NX, 64, 2048), BF16),
            pltpu.VMEM((2, 32, 2048), BF16),
            pltpu.VMEM((2, 64, 2048), BF16),
            sem((9,)),
            sem((9,)),
            sem((9,)),
            sem((3, 2, 8)),
            sem((3, 2, 8)),
            sem((2, 16)),
            sem((2, 16)),
            sem((2, 16)),
            sem((2, 16)),
            sem((2, CH1)),
            sem((2, CH1)),
            sem((2, CH1)),
            sem((2, CH1)),
            sem((2, CH2)),
            sem((2, CH2)),
            sem((2, CH2)),
            sem((2, CH2)),
            sem((2, 2, 8)),
            sem((2, 2, 8)),
            sem((2,)),
            sem((2,)),
            sem((7,)),
            sem((7,)),
        ],
        compiler_params=pltpu.CompilerParams(
            collective_id=0, has_side_effects=True, vmem_limit_bytes=60 * 1024 * 1024
        ),
    )(
        inputs[0], query_weight, key_weight, value_weight, post_gate_weight,
        pre_gate_weight, inner_weight, attn_out_weight, conv_out_weight,
        norm_gain.reshape(1, -1),
        jnp.tile(query_gain, 2).reshape(1, -1),
        jnp.tile(key_gain, 2).reshape(1, -1),
        head_gain.reshape(1, -1),
        conv_taps,
        mix_lambda,
    )
    return out[None]


def solution(mesh):
    rows = P(("sp", "fs"), "tp")
    placed = (
        P("fs", "sp", "tp"), P(), rows, rows, rows, P(), P(), P(), P(),
        rows, rows, rows, P(), rows, rows,
    )
    return jax.shard_map(
        per_device,
        mesh=mesh,
        in_specs=placed,
        out_specs=P("fs", ("sp", "tp"), None),
        check_vma=False,
    )
```

```python
import functools

import jax
import jax.numpy as jnp
from jax import lax
from jax.experimental import pallas as pl
from jax.experimental.pallas import tpu as pltpu
from jax.sharding import PartitionSpec as P

EPS = 1e-06
MESH = pl.DeviceIdType.MESH
F32 = jnp.float32
BF16 = jnp.bfloat16
LOG2E = 1.4426950408889634

NZ, NY, NX = 16, 4, 4


def body(
    tok_ref, wq_ref, wk_ref, wv_ref, wpost_ref, wpre_ref, winner_ref, wao_ref, wco_ref,
    ngain_ref, qgain_ref, kgain_ref, hgain_ref, taps_ref, lam_ref,
    out_ref,
    xg, nrm, w0, wa, w2, w3, kb, vb, qb, m_s, l_s, acc_s, hid, ah, conv, sigb, sigf, halo, postb,
    part, pair_in, psum, rel, fin,
    lsem, xss, xrs, xas, xar, zss, zrs, yds, ydr, yfs, yfr,
    kvs, kvr, hs, hr, rs, rr, als, alr,
):
    z = lax.axis_index("sp")
    y = lax.axis_index("fs")
    t = lax.axis_index("tp")
    x = t // 2
    c = t % 2

    def zz(i):
        return (i + 2 * NZ) % NZ

    def yy(i):
        return (i + 2 * NY) % NY

    def xx(i):
        return (i + 2 * NX) % NX

    dev_z = ({"sp": zz(z + 1)}, {"sp": zz(z - 1)})
    dev_zz = ({"sp": zz(z + 2)}, {"sp": zz(z - 2)})
    dev_y = ({"fs": yy(y + 1)}, {"fs": yy(y - 1)})
    dev_x = ({"tp": xx(x + 1) * 2 + c}, {"tp": xx(x - 1) * 2 + c})
    other = x * 2 + (1 - c)
    dev_c = {"tp": other}
    group = tuple({"tp": (t + i) % 8} for i in range(1, 8))
    peers = dev_z + dev_zz + dev_y + group

    def rc(src, dst, ssem, rsem, dev):
        return pltpu.make_async_remote_copy(
            src_ref=src, dst_ref=dst, send_sem=ssem, recv_sem=rsem,
            device_id=dev, device_id_type=MESH,
        )

    own = (
        (tok_ref, xg.at[t]),
        (wq_ref, w0.at[z, y, :, 0:128]),
        (wk_ref, w0.at[z, y, :, 128:256]),
        (wv_ref, w0.at[z, y, :, 256:384]),
        (wao_ref, wa.at[t, z, y]),
        (wpost_ref, w2.at[z, y, :, 0:256]),
        (wpre_ref, w2.at[z, y, :, 256:512]),
        (winner_ref, w2.at[z, y, :, 512:768]),
        (wco_ref, w3.at[z, y]),
    )
    local = [pltpu.make_async_copy(s, d, lsem.at[i]) for i, (s, d) in enumerate(own)]
    for cp in local:
        cp.start()
    barrier = pltpu.get_barrier_semaphore()
    for dev in peers:
        pl.semaphore_signal(barrier, inc=1, device_id=dev, device_id_type=MESH)

    qb[...] = jnp.zeros_like(qb)
    m_s[...] = jnp.full_like(m_s, -1e30)
    l_s[...] = jnp.zeros_like(l_s)
    acc_s[...] = jnp.zeros_like(acc_s)

    pl.semaphore_wait(barrier, len(peers))

    own_wa = wa.at[t]
    ws = (w0, own_wa, w2, w3)
    zsteps = ((7, 8), (8, 7), (7, 8), (8, 7))

    def z_slab(d, s):
        return zz(z - s) if d == 0 else zz(z + s)

    def z_copy(g, d, s, stride=1):
        ref = ws[g].at[z_slab(d, s - stride), y]
        dev = (dev_z if stride == 1 else dev_zz)[d]
        return rc(ref, ref, zss.at[g, d, s - 1], zrs.at[g, d, s - 1], dev)

    def z_wait(g, d, s):
        ref = ws[g].at[z_slab(d, s), y]
        rc(ref, ref, zss.at[g, d, s - 1], zrs.at[g, d, s - 1], dev_z[d]).wait_recv()

    def z_serve(s):
        for g in (2, 3):
            for d in range(2):
                if s <= zsteps[g][d]:
                    z_wait(g, d, s)
                    if s < zsteps[g][d]:
                        z_copy(g, d, s + 1).start()

    def level(s):
        return (0,) if s == 0 else (15,) if s == 8 else (2 * s - 1, 2 * s)

    def slab_at(k):
        return zz(z + (k + 1) // 2 * (1 - 2 * (k % 2)))

    def y_direct(g, k, d, mine):
        col = y if mine else yy(y - 1) if d == 0 else yy(y + 1)
        ref = ws[g].at[slab_at(k), col]
        return rc(ref, ref, yds.at[g, d, k], ydr.at[g, d, k], dev_y[d])

    def y_half(g, k, d, mine):
        col = yy(y + 2) if not mine else yy(y - 1) if d == 0 else yy(y + 1)
        ref = ws[g].at[slab_at(k), col, pl.ds(16 * d, 16)]
        return rc(ref, ref, yfs.at[g, d, k], yfr.at[g, d, k], dev_y[d])

    def y_send(g, *steps):
        for s in steps:
            for k in level(s):
                for d in range(2):
                    y_direct(g, k, d, True).start()

    def y_relay(g, *steps):
        for s in steps:
            for k in level(s):
                for d in range(2):
                    y_direct(g, k, d, False).wait_recv()
                    y_half(g, k, d, True).start()

    def y_done(g, *steps):
        for s in steps:
            for k in level(s):
                for d in range(2):
                    y_half(g, k, d, False).wait_recv()

    left, right, far = xx(x - 1), xx(x + 1), xx(x + 2)

    def x_gather(buf, lo, hi, ss, sr, start):
        def send(k, slot, dev, piece=None):
            ref = buf.at[slot] if piece is None else buf.at[slot, piece]
            start(rc(ref, ref, ss.at[k], sr.at[k], dev))

        def wait(k, slot, piece=None):
            ref = buf.at[slot] if piece is None else buf.at[slot, piece]
            rc(ref, ref, ss.at[k], sr.at[k], dev_c).wait_recv()

        def begin():
            send(0, t, dev_x[0])
            send(1, t, dev_x[1])
            send(2, t, dev_c)

        def middle():
            wait(0, left * 2 + c)
            send(5, left * 2 + c, dev_x[0], lo)
            wait(1, right * 2 + c)
            send(6, right * 2 + c, dev_x[1], hi)
            send(3, left * 2 + c, dev_c)
            send(4, right * 2 + c, dev_c)

        def late():
            wait(5, far * 2 + c, lo)
            send(7, far * 2 + c, dev_c, lo)
            wait(6, far * 2 + c, hi)
            send(8, far * 2 + c, dev_c, hi)

        def finish():
            wait(2, other)
            wait(3, left * 2 + (1 - c))
            wait(4, right * 2 + (1 - c))
            wait(7, far * 2 + (1 - c), lo)
            wait(8, far * 2 + (1 - c), hi)

        def drain():
            for k, slot, piece in (
                (0, t, None), (1, t, None), (2, t, None),
                (5, left * 2 + c, lo), (6, right * 2 + c, hi),
                (3, left * 2 + c, None), (4, right * 2 + c, None),
                (7, far * 2 + c, lo), (8, far * 2 + c, hi),
            ):
                ref = buf.at[slot] if piece is None else buf.at[slot, piece]
                rc(ref, ref, ss.at[k], sr.at[k], dev_c).wait_send()

        return begin, middle, late, finish, drain

    x_begin, x_service_a, x_service_b, x_finish, x_drain = x_gather(
        xg, pl.ds(0, 256), pl.ds(256, 256), xss, xrs, lambda copy: copy.start()
    )
    a_begin, a_middle, a_late, a_finish, a_drain = x_gather(
        wa, pl.ds(0, 8), pl.ds(8, 8), xas, xar, lambda copy: copy.start()
    )

    for i in (1, 2, 3):
        local[i].wait()
    for stride in (1, 2):
        for d in range(2):
            z_copy(0, d, stride, stride).start()
    local[0].wait()
    x_begin()
    y_send(0, 0)
    local[4].wait()
    for stride in (1, 2):
        for d in range(2):
            z_copy(1, d, stride, stride).start()
    y_send(1, 0)
    for i in range(5, 9):
        local[i].wait()
    for g in (2, 3):
        for d in range(2):
            z_copy(g, d, 1).start()

    def normalize():
        def tile(i, carry):
            rows = pl.ds(pl.multiple_of(i * 32, 32), 32)
            total = jnp.zeros((32, 256), F32)
            for b in range(8):
                v = xg[b, rows, :].astype(F32)
                total = total + v * v
            r = lax.rsqrt(jnp.sum(total, axis=-1, keepdims=True) * (1.0 / 2048) + EPS)
            for b in range(8):
                v = xg[b, rows, :].astype(F32) * r * ngain_ref[:, b * 256 : (b + 1) * 256]
                nrm[rows, b * 256 : (b + 1) * 256] = v.astype(BF16)
            return carry

        lax.fori_loop(0, 16, tile, 0)

    def z_round(r):
        for g in (0, 1):
            for s in (2 * r - 1, 2 * r):
                for d in range(2):
                    if s <= zsteps[g][d]:
                        z_wait(g, d, s)
                        if s + 2 <= zsteps[g][d]:
                            z_copy(g, d, s + 2, 2).start()
                y_send(g, s)

    z_round(1)
    y_relay(0, 0)
    z_serve(1)
    z_round(2)
    y_relay(0, 1, 2)
    y_relay(1, 0)
    z_serve(2)
    x_service_a()
    z_round(3)
    y_relay(0, 3, 4)
    y_relay(1, 1, 2)
    z_serve(3)
    z_round(4)
    y_relay(0, 5, 6)
    x_service_b()
    y_relay(0, 7, 8)
    y_relay(1, 3, 4)
    y_send(2, 0)
    z_serve(4)
    x_finish()
    normalize()
    z_serve(5)
    y_relay(1, 5, 6)
    y_send(2, 1, 2)
    y_done(0, *range(9))

    lane = lax.broadcasted_iota(jnp.int32, (128, 128), 1)
    first = lane < 64

    def half_norm(v, gain):
        sq = v * v
        s1 = jnp.sum(jnp.where(first, sq, 0.0), axis=-1, keepdims=True)
        s2 = jnp.sum(jnp.where(first, 0.0, sq), axis=-1, keepdims=True)
        r = jnp.where(
            first, lax.rsqrt(s1 * (1.0 / 64) + EPS), lax.rsqrt(s2 * (1.0 / 64) + EPS)
        )
        return v * r * gain

    kgain = jnp.concatenate([kgain_ref[...]] * 2, axis=1)
    qgain = jnp.concatenate([qgain_ref[...]] * 2, axis=1)

    def kv_tile(i, carry):
        rows = pl.ds(pl.multiple_of(i * 128, 128), 128)
        kv = jnp.dot(
            nrm[rows, :], w0[:, :, :, 128:384].reshape(2048, 256), preferred_element_type=F32
        )
        kb[z, rows, :] = half_norm(kv[:, 0:128], kgain).astype(BF16)
        vb[z, :, rows] = kv[:, 128:256].T.astype(BF16)
        return carry

    def q_tile(i, carry):
        rows = pl.ds(pl.multiple_of(i * 128, 128), 128)
        rows2 = pl.ds(pl.multiple_of(i * 128 + 512, 128), 128)
        q = jnp.dot(
            nrm[rows, :], w0[:, :, :, 0:128].reshape(2048, 128), preferred_element_type=F32
        )
        qt = half_norm(q, qgain).T.astype(BF16)
        qb[0:64, rows] = qt[0:64]
        qb[64:128, rows2] = qt[64:128]
        return carry

    lax.fori_loop(0, 4, kv_tile, 0)

    bufs = (kb, vb)

    def kv_copy(d, w, s):
        i = zz(z - (s - 1)) if d == 0 else zz(z + (s - 1))
        ref = bufs[w].at[i]
        return rc(ref, ref, kvs.at[d, w, s - 1], kvr.at[d, w, s - 1], dev_z[d])

    def kv_wait(d, w, s):
        i = zz(z - s) if d == 0 else zz(z + s)
        ref = bufs[w].at[i]
        rc(ref, ref, kvs.at[d, w, s - 1], kvr.at[d, w, s - 1], dev_z[d]).wait_recv()

    for w in range(2):
        for d in range(2):
            kv_copy(d, w, 1).start()

    factor = LOG2E * 0.125

    y_relay(1, 7, 8)
    y_relay(2, 0)
    y_send(2, 3)
    lax.fori_loop(0, 4, q_tile, 0)

    def attend(b):
        def pair(j, carry):
            cols = [pl.ds(pl.multiple_of(j * 512 + i * 256, 256), 256) for i in range(2)]
            st = [jnp.dot(kb[b], qb[:, cs], preferred_element_type=F32) for cs in cols]
            for i, cs in enumerate(cols):
                m_old = m_s[:, cs]
                m_new = jnp.maximum(m_old, jnp.max(st[i], axis=0, keepdims=True))
                p = jnp.exp2((st[i] - m_new) * factor)
                a = jnp.exp2((m_old - m_new) * factor)
                l_s[:, cs] = l_s[:, cs] * a + jnp.sum(p, axis=0, keepdims=True)
                acc_s[:, cs] = acc_s[:, cs] * a + jnp.dot(
                    vb[b], p.astype(BF16), preferred_element_type=F32
                )
                m_s[:, cs] = m_new
            return carry

        lax.fori_loop(0, 2, pair, 0)

    def conv_project():
        def tile(i, carry):
            rows = pl.ds(pl.multiple_of(i * 128, 128), 128)
            rows8 = pl.ds(pl.multiple_of(i * 128 + 8, 8), 128)
            r = jnp.dot(nrm[rows, :], w2[...].reshape(2048, 768), preferred_element_type=F32)
            postb[rows, :] = r[:, 0:256].astype(BF16)
            signal = (r[:, 256:512] * r[:, 512:768]).astype(BF16)
            sigb[rows, :] = signal
            sigf[rows8, :] = signal.astype(F32)
            return carry

        lax.fori_loop(0, 4, tile, 0)

    def halo_copy(d):
        src = sigb.at[pl.ds(496, 16)] if d == 0 else sigb.at[pl.ds(0, 16)]
        return rc(src, halo.at[d], hs.at[d], hr.at[d], dev_z[d])

    def conv_filter():
        before = halo[0].astype(F32)[8:16]
        after = halo[1].astype(F32)[0:8]
        sigf[0:8, :] = jnp.where(z > 0, before, 0.0)
        sigf[520:528, :] = jnp.where(z < NZ - 1, after, 0.0)
        taps = taps_ref[:, pl.ds(pl.multiple_of(t * 256, 256), 256)]
        for i in range(4):
            r = i * 128
            filtered = (
                taps[0:1] * sigf[r + 7 : r + 135, :]
                + taps[1:2] * sigf[r + 8 : r + 136, :]
                + taps[2:3] * sigf[r + 9 : r + 137, :]
            )
            conv[r : r + 128, :] = (
                postb[r : r + 128, :].astype(F32) * filtered
            ).astype(BF16)

    up, down = pl.ds(0, 32), pl.ds(32, 32)

    def conv_out():
        def tile(n, carry):
            cols = pl.ds(pl.multiple_of(n * 256, 256), 256)
            r = lax.dot_general(
                conv[...], w3[pl.ds(n * 2, 2)].reshape(256, 256),
                (((1,), (1,)), ((), ())), preferred_element_type=F32,
            )
            part[:, :, :, cols] = r.astype(BF16).reshape(NX, 2, 64, 256)
            return carry

        lax.fori_loop(0, 8, tile, 0)

    sums = (
        lambda: rc(part.at[:, 1 - c], pair_in, rs.at[0], rr.at[0], dev_c),
        lambda: rc(psum.at[far, up], rel.at[0], rs.at[1], rr.at[1], dev_x[0]),
        lambda: rc(psum.at[far, down], rel.at[1], rs.at[2], rr.at[2], dev_x[1]),
        lambda: rc(psum.at[right, down], fin.at[0, down], rs.at[3], rr.at[3], dev_x[0]),
        lambda: rc(psum.at[left, up], fin.at[1, up], rs.at[4], rr.at[4], dev_x[1]),
        lambda: rc(psum.at[right, up], fin.at[0, up], rs.at[5], rr.at[5], dev_x[0]),
        lambda: rc(psum.at[left, down], fin.at[1, down], rs.at[6], rr.at[6], dev_x[1]),
    )

    def sum_pair(j):
        psum[j] = (part[j, c].astype(F32) + pair_in[j].astype(F32)).astype(BF16)

    def sum_first():
        sums[0]().wait_recv()
        sum_pair(far)
        sums[1]().start()
        sums[2]().start()
        sum_pair(right)
        sum_pair(left)
        sums[3]().start()
        sums[4]().start()

    def sum_second():
        sums[1]().wait_recv()
        psum[right, 0:32] = (psum[right, 0:32].astype(F32) + rel[0].astype(F32)).astype(BF16)
        sums[5]().start()
        sums[2]().wait_recv()
        psum[left, 32:64] = (psum[left, 32:64].astype(F32) + rel[1].astype(F32)).astype(BF16)
        sums[6]().start()

    def relay(w, s):
        for d in range(2):
            kv_wait(d, w, s)
            if d == w:
                kv_copy(d, w, s + 1).start()
            else:

                @pl.when(s < 7)
                def _():
                    kv_copy(d, w, s + 1).start()

    def conv_send():
        conv_project()
        for d in range(2):
            halo_copy(d).start()

    def conv_finish():
        for d in range(2):
            halo_copy(d).wait_recv()
        conv_filter()

    def conv_sum():
        y_done(3, *range(9))
        conv_out()
        sums[0]().start()

    jobs = {
        (1, 0): lambda: (y_send(2, 4), y_relay(2, 1), y_done(1, *range(9)), a_begin()),
        (1, 1): lambda: (z_serve(6), y_relay(2, 2), y_send(2, 5)),
        (2, 0): lambda: (y_relay(2, 3),),
        (2, 1): lambda: (z_serve(7), y_send(2, 6), y_relay(2, 4)),
        (3, 0): lambda: (y_relay(2, 5),),
        (3, 1): lambda: (z_serve(8), y_send(2, 7), y_relay(2, 6), a_middle()),
        (4, 0): lambda: (y_send(2, 8), y_send(3, 0, 1, 2), y_relay(2, 7)),
        (4, 1): lambda: (y_relay(2, 8), y_send(3, 3, 4, 5, 6, 7, 8)),
        (5, 0): lambda: (y_relay(3, 0, 1, 2), a_late()),
        (5, 1): lambda: (y_relay(3, 3, 4, 5), y_done(2, *range(9)), conv_send()),
        (6, 0): lambda: (y_relay(3, 6, 7, 8),),
        (6, 1): lambda: (conv_finish(), conv_sum()),
        (7, 1): lambda: (sum_first(), a_finish()),
    }

    def serve(s, w):
        for (at, half), job in jobs.items():
            if half == w:

                @pl.when(s == at)
                def _(job=job):
                    job()

    relay(0, 1)
    jobs[1, 0]()
    relay(1, 1)
    jobs[1, 1]()
    attend(z)

    def kv_step(s, carry):
        relay(0, s)
        serve(s, 0)
        attend(zz(z - (s - 1)))
        relay(1, s)
        serve(s, 1)
        attend(zz(z + (s - 1)))
        return carry

    lax.fori_loop(2, 8, kv_step, 0)
    attend(zz(z - 7))
    attend(zz(z + 7))
    sum_second()
    kv_wait(0, 0, 8)
    kv_wait(1, 1, 8)
    attend(zz(z + 8))

    lam = lam_ref[t]
    inv = 1.0 / l_s[...]
    head = acc_s[:, 0:512] * inv[:, 0:512] - lam * (acc_s[:, 512:1024] * inv[:, 512:1024])
    r = lax.rsqrt(jnp.sum(head * head, axis=0, keepdims=True) * (1.0 / 128) + EPS)
    hid[...] = ((head * r).T * hgain_ref[...]).astype(BF16)

    def give(i):
        peer = (t + i) % 8
        rows = pl.ds(pl.multiple_of(peer * 64, 64), 64)
        return rc(hid.at[rows], ah.at[t], als.at[i - 1], alr.at[i - 1], {"tp": peer})

    for i in range(1, 8):
        give(i).start()
    ah[t] = hid[pl.ds(pl.multiple_of(t * 64, 64), 64), :]
    for k in (3, 4, 5, 6):
        sums[k]().wait_recv()
    mine = part[x, c].astype(F32) + pair_in[x].astype(F32)
    acc_o = mine + fin[0].astype(F32) + fin[1].astype(F32)
    for i in range(1, 8):
        source = (t + 8 - i) % 8
        rc(ah.at[source], ah.at[source], als.at[i - 1], alr.at[i - 1], dev_c).wait_recv()
    whole = jnp.concatenate([ah[i] for i in range(8)], axis=1)
    for n in range(8):
        w = jnp.concatenate(
            [wa[i, 2 * n : 2 * n + 2].reshape(256, 128) for i in range(8)], axis=1
        )
        r = lax.dot_general(whole, w, (((1,), (1,)), ((), ())), preferred_element_type=F32)
        cols = slice(n * 256, n * 256 + 256)
        out_ref[:, cols] = (acc_o[:, cols] + r).astype(BF16)

    for g in range(4):
        for d in range(2):
            for step in range(1, zsteps[g][d] + 1):
                z_copy(g, d, step, 2 if g < 2 and step > 1 else 1).wait_send()

    def y_drain(k, carry):
        for g in range(4):
            for d in range(2):
                y_direct(g, k, d, True).wait_send()
                y_half(g, k, d, True).wait_send()
        return carry

    lax.fori_loop(0, 16, y_drain, 0)
    for w in range(2):
        for d in range(2):
            for s in range(1, 9 if d == w else 8):
                kv_copy(d, w, s).wait_send()
    x_drain()
    a_drain()
    for d in range(2):
        halo_copy(d).wait_send()
    for make in sums:
        make().wait_send()
    for i in range(1, 8):
        give(i).wait_send()


def per_device(
    inputs, norm_gain, query_weight, key_weight, value_weight, query_gain, key_gain,
    mix_lambda, head_gain, post_gate_weight, pre_gate_weight, inner_weight, conv_taps,
    attn_out_weight, conv_out_weight,
):
    hbm = pl.BlockSpec(memory_space=pl.ANY)
    vmem = pl.BlockSpec(memory_space=pltpu.VMEM)
    smem = pl.BlockSpec(memory_space=pltpu.SMEM)
    sem = pltpu.SemaphoreType.DMA
    out = pl.pallas_call(
        body,
        out_shape=jax.ShapeDtypeStruct((64, 2048), BF16),
        in_specs=[hbm] * 9 + [vmem] * 5 + [smem],
        out_specs=vmem,
        scratch_shapes=[
            pltpu.VMEM((8, 512, 256), BF16),
            pltpu.VMEM((512, 2048), BF16),
            pltpu.VMEM((NZ, NY, 32, 384), BF16),
            pltpu.VMEM((8, NZ, NY, 32, 128), BF16),
            pltpu.VMEM((NZ, NY, 32, 768), BF16),
            pltpu.VMEM((NZ, NY, 32, 256), BF16),
            pltpu.VMEM((NZ, 512, 128), BF16),
            pltpu.VMEM((NZ, 128, 512), BF16),
            pltpu.VMEM((128, 1024), BF16),
            pltpu.VMEM((1, 1024), F32),
            pltpu.VMEM((1, 1024), F32),
            pltpu.VMEM((128, 1024), F32),
            pltpu.VMEM((512, 128), BF16),
            pltpu.VMEM((8, 64, 128), BF16),
            pltpu.VMEM((512, 256), BF16),
            pltpu.VMEM((512, 256), BF16),
            pltpu.VMEM((528, 256), F32),
            pltpu.VMEM((2, 16, 256), BF16),
            pltpu.VMEM((512, 256), BF16),
            pltpu.VMEM((NX, 2, 64, 2048), BF16),
            pltpu.VMEM((NX, 64, 2048), BF16),
            pltpu.VMEM((NX, 64, 2048), BF16),
            pltpu.VMEM((2, 32, 2048), BF16),
            pltpu.VMEM((2, 64, 2048), BF16),
            sem((9,)),
            sem((9,)),
            sem((9,)),
            sem((9,)),
            sem((9,)),
            sem((4, 2, 8)),
            sem((4, 2, 8)),
            sem((4, 2, 16)),
            sem((4, 2, 16)),
            sem((4, 2, 16)),
            sem((4, 2, 16)),
            sem((2, 2, 8)),
            sem((2, 2, 8)),
            sem((2,)),
            sem((2,)),
            sem((7,)),
            sem((7,)),
            sem((7,)),
            sem((7,)),
        ],
        compiler_params=pltpu.CompilerParams(
            collective_id=0, has_side_effects=True, vmem_limit_bytes=60 * 1024 * 1024
        ),
    )(
        inputs[0], query_weight, key_weight, value_weight, post_gate_weight,
        pre_gate_weight, inner_weight, attn_out_weight, conv_out_weight,
        norm_gain.reshape(1, -1),
        query_gain.reshape(1, -1),
        key_gain.reshape(1, -1),
        head_gain.reshape(1, -1),
        conv_taps,
        mix_lambda,
    )
    return out[None]


def solution(mesh):
    rows = P(("sp", "fs"), "tp")
    placed = (
        P("fs", "sp", "tp"), P(), rows, rows, rows, P(), P(), P(), P(),
        rows, rows, rows, P(), rows, rows,
    )
    return jax.shard_map(
        per_device,
        mesh=mesh,
        in_specs=placed,
        out_specs=P("fs", ("sp", "tp"), None),
        check_vma=False,
    )
```

```python
import functools

import jax
import jax.numpy as jnp
from jax import lax
from jax.experimental import pallas as pl
from jax.experimental.pallas import tpu as pltpu
from jax.sharding import PartitionSpec as P

EPS = 1e-06
MESH = pl.DeviceIdType.MESH
F32 = jnp.float32
BF16 = jnp.bfloat16
LOG2E = 1.4426950408889634

NZ, NY, NX = 16, 4, 4


def body(
    tok_ref, wq_ref, wk_ref, wv_ref, wpost_ref, wpre_ref, winner_ref, wao_ref, wco_ref,
    ngain_hbm, qgain_hbm, kgain_hbm, hgain_hbm, taps_hbm, lam_hbm,
    out_ref,
    ngain_ref, qgain_ref, kgain_ref, hgain_ref, taps_ref, lam_ref,
    xg, nrm, w0, w1, wa, w2, w3, kb, vb, qb, m_s, l_s, acc_s, hid, ah, conv, sigb, sigf, halo, postb,
    part, pair_in, psum, rel, fin, acc_o,
    lsem, xss, xrs, xas, xar, zss, zrs, yds, ydr, yfs, yfr,
    kvs, kvr, hs, hr, rs, rr, als, alr,
):
    z = lax.axis_index("sp")
    y = lax.axis_index("fs")
    t = lax.axis_index("tp")
    x = t // 2
    c = t % 2

    def zz(i):
        return (i + 2 * NZ) % NZ

    def yy(i):
        return (i + 2 * NY) % NY

    def xx(i):
        return (i + 2 * NX) % NX

    dev_z = ({"sp": zz(z + 1)}, {"sp": zz(z - 1)})
    dev_zz = ({"sp": zz(z + 2)}, {"sp": zz(z - 2)})
    dev_y = ({"fs": yy(y + 1)}, {"fs": yy(y - 1)})
    dev_x = ({"tp": xx(x + 1) * 2 + c}, {"tp": xx(x - 1) * 2 + c})
    other = x * 2 + (1 - c)
    dev_c = {"tp": other}
    group = tuple({"tp": (t + i) % 8} for i in range(1, 8))
    dev_far = {"fs": yy(y + 2)}
    peers = dev_z + dev_zz + dev_y + (dev_far,) + group

    def rc(src, dst, ssem, rsem, dev):
        return pltpu.make_async_remote_copy(
            src_ref=src, dst_ref=dst, send_sem=ssem, recv_sem=rsem,
            device_id=dev, device_id_type=MESH,
        )

    own = (
        (tok_ref, xg.at[t]),
        (wk_ref, w0.at[z, y, :, 0:128]),
        (wv_ref, w0.at[z, y, :, 128:256]),
        (wq_ref, w1.at[z, y]),
        (wao_ref, wa.at[t, z, y]),
        (wpost_ref, w2.at[z, y, :, 0:256]),
        (wpre_ref, w2.at[z, y, :, 256:512]),
        (winner_ref, w2.at[z, y, :, 512:768]),
        (wco_ref, w3.at[z, y]),
        (ngain_hbm, ngain_ref),
        (qgain_hbm, qgain_ref),
        (kgain_hbm, kgain_ref),
        (hgain_hbm, hgain_ref),
        (taps_hbm, taps_ref),
        (lam_hbm, lam_ref),
    )
    local = [pltpu.make_async_copy(s, d, lsem.at[i]) for i, (s, d) in enumerate(own)]
    for cp in local:
        cp.start()
    barrier = pltpu.get_barrier_semaphore()
    for dev in peers:
        pl.semaphore_signal(barrier, inc=1, device_id=dev, device_id_type=MESH)

    qb[...] = jnp.zeros_like(qb)
    m_s[...] = jnp.full_like(m_s, -1e30)
    l_s[...] = jnp.zeros_like(l_s)
    acc_s[...] = jnp.zeros_like(acc_s)

    pl.semaphore_wait(barrier, len(peers))

    own_wa = wa.at[t]
    ws = (w0, w1, w2, w3, own_wa)
    zsteps = ((7, 8), (8, 7), (7, 8), (8, 7), (8, 7))

    def z_slab(d, s):
        return zz(z - s) if d == 0 else zz(z + s)

    def z_copy(g, d, s, stride=1):
        ref = ws[g].at[z_slab(d, s - stride), y]
        dev = (dev_z if stride == 1 else dev_zz)[d]
        return rc(ref, ref, zss.at[g, d, s - 1], zrs.at[g, d, s - 1], dev)

    def z_wait(g, d, s):
        ref = ws[g].at[z_slab(d, s), y]
        rc(ref, ref, zss.at[g, d, s - 1], zrs.at[g, d, s - 1], dev_z[d]).wait_recv()

    def z_serve(s):
        for g in (2, 3):
            for d in range(2):
                if s <= zsteps[g][d]:
                    z_wait(g, d, s)
                    if s < zsteps[g][d]:
                        z_copy(g, d, s + 1).start()

    def level(s):
        return (0,) if s == 0 else (15,) if s == 8 else (2 * s - 1, 2 * s)

    def slab_at(k):
        return zz(z + (k + 1) // 2 * (1 - 2 * (k % 2)))

    def y_direct(g, k, d, mine):
        col = y if mine else yy(y - 1) if d == 0 else yy(y + 1)
        ref = ws[g].at[slab_at(k), col]
        return rc(ref, ref, yds.at[g, d, k], ydr.at[g, d, k], dev_y[d])

    def y_half(g, k, d, mine):
        col = yy(y + 2) if not mine else yy(y - 1) if d == 0 else yy(y + 1)
        ref = ws[g].at[slab_at(k), col, pl.ds(16 * d, 16)]
        return rc(ref, ref, yfs.at[g, d, k], yfr.at[g, d, k], dev_y[d])

    def y_send(g, *steps):
        for s in steps:
            for k in level(s):
                for d in range(2):
                    y_direct(g, k, d, True).start()

    def y_relay(g, *steps):
        for s in steps:
            for k in level(s):
                for d in range(2):
                    y_direct(g, k, d, False).wait_recv()
                    y_half(g, k, d, True).start()

    def y_far(g, k, mine):
        ref = ws[g].at[slab_at(k), y if mine else yy(y + 2)]
        return rc(ref, ref, yfs.at[g, 0, k], yfr.at[g, 0, k], dev_far)

    def y_done(g, *steps):
        for s in steps:
            for k in level(s):
                for d in range(2):
                    y_half(g, k, d, False).wait_recv()

    left, right, far = xx(x - 1), xx(x + 1), xx(x + 2)

    def x_gather(buf, lo, hi, ss, sr, start):
        def send(k, slot, dev, piece=None):
            ref = buf.at[slot] if piece is None else buf.at[slot, piece]
            start(rc(ref, ref, ss.at[k], sr.at[k], dev))

        def wait(k, slot, piece=None):
            ref = buf.at[slot] if piece is None else buf.at[slot, piece]
            rc(ref, ref, ss.at[k], sr.at[k], dev_c).wait_recv()

        def begin():
            send(0, t, dev_x[0])
            send(1, t, dev_x[1])
            send(2, t, dev_c)

        def middle():
            wait(0, left * 2 + c)
            send(5, left * 2 + c, dev_x[0], lo)
            wait(1, right * 2 + c)
            send(6, right * 2 + c, dev_x[1], hi)
            send(3, left * 2 + c, dev_c)
            send(4, right * 2 + c, dev_c)

        def late():
            wait(5, far * 2 + c, lo)
            send(7, far * 2 + c, dev_c, lo)
            wait(6, far * 2 + c, hi)
            send(8, far * 2 + c, dev_c, hi)

        def finish():
            wait(2, other)
            wait(3, left * 2 + (1 - c))
            wait(4, right * 2 + (1 - c))
            wait(7, far * 2 + (1 - c), lo)
            wait(8, far * 2 + (1 - c), hi)

        def drain():
            for k, slot, piece in (
                (0, t, None), (1, t, None), (2, t, None),
                (5, left * 2 + c, lo), (6, right * 2 + c, hi),
                (3, left * 2 + c, None), (4, right * 2 + c, None),
                (7, far * 2 + c, lo), (8, far * 2 + c, hi),
            ):
                ref = buf.at[slot] if piece is None else buf.at[slot, piece]
                rc(ref, ref, ss.at[k], sr.at[k], dev_c).wait_send()

        return begin, middle, late, finish, drain

    x_begin, x_service_a, x_service_b, x_finish, x_drain = x_gather(
        xg, pl.ds(0, 256), pl.ds(256, 256), xss, xrs, lambda copy: copy.start()
    )
    a_begin, a_middle, a_late, a_finish, a_drain = x_gather(
        wa, pl.ds(0, 8), pl.ds(8, 8), xas, xar, lambda copy: copy.start()
    )

    for i in (1, 2):
        local[i].wait()
    for stride in (1, 2):
        for d in range(2):
            z_copy(0, d, stride, stride).start()
    local[0].wait()
    x_begin()
    y_send(0, 0)
    local[3].wait()
    for stride in (1, 2):
        for d in range(2):
            z_copy(1, d, stride, stride).start()
    for i in range(4, 9):
        local[i].wait()
    for stride in (1, 2):
        for d in range(2):
            z_copy(4, d, stride, stride).start()
    for g in (2, 3):
        for d in range(2):
            z_copy(g, d, 1).start()
    for i in range(9, len(local)):
        local[i].wait()

    def normalize():
        def tile(i, carry):
            rows = pl.ds(pl.multiple_of(i * 32, 32), 32)
            total = jnp.zeros((32, 256), F32)
            for b in range(8):
                v = xg[b, rows, :].astype(F32)
                total = total + v * v
            r = lax.rsqrt(jnp.sum(total, axis=-1, keepdims=True) * (1.0 / 2048) + EPS)
            for b in range(8):
                v = xg[b, rows, :].astype(F32) * r * ngain_ref[:, b * 256 : (b + 1) * 256]
                nrm[rows, b * 256 : (b + 1) * 256] = v.astype(BF16)
            return carry

        lax.fori_loop(0, 16, tile, 0)

    def z_strides(g, r):
        for s in (2 * r - 1, 2 * r):
            for d in range(2):
                if s <= zsteps[g][d]:
                    z_wait(g, d, s)
                    if s + 2 <= zsteps[g][d]:
                        z_copy(g, d, s + 2, 2).start()

    def z_round(r):
        z_strides(0, r)
        y_send(0, 2 * r - 1, 2 * r)
        z_strides(1, r)
        if r > 1:
            z_strides(4, r - 1)

    far_slabs = level(7) + level(8)

    z_round(1)
    y_relay(0, 0)
    y_send(1, 0)
    y_send(2, 0)
    z_serve(1)
    z_round(2)
    x_service_a()
    y_relay(0, 1, 2)
    y_send(1, 1, 2)
    y_send(2, 1)
    z_serve(2)
    z_round(3)
    y_relay(0, 3, 4)
    y_relay(1, 0, 1)
    y_send(1, 3)
    y_send(4, 0, 1, 2)
    y_relay(2, 0)
    z_serve(3)
    z_round(4)
    for k in far_slabs:
        y_far(0, k, True).start()
    x_service_b()
    y_relay(0, 5, 6)
    z_serve(4)
    y_send(1, 4, 5, 6, 7, 8)
    y_send(4, 3, 4)
    x_finish()
    normalize()
    z_strides(4, 4)
    y_relay(1, 2, 3)
    y_relay(2, 1)
    y_relay(4, 0, 1)
    y_send(4, 5, 6, 7, 8)
    y_done(0, *range(7))
    for k in far_slabs:
        y_far(0, k, False).wait_recv()
        for d in range(2):
            y_direct(0, k, d, False).wait_recv()

    def half_norm(v, gain):
        first = lax.broadcasted_iota(jnp.int32, v.shape, 1) < 64
        sq = v * v
        s1 = jnp.sum(jnp.where(first, sq, 0.0), axis=-1, keepdims=True)
        s2 = jnp.sum(jnp.where(first, 0.0, sq), axis=-1, keepdims=True)
        r = jnp.where(
            first, lax.rsqrt(s1 * (1.0 / 64) + EPS), lax.rsqrt(s2 * (1.0 / 64) + EPS)
        )
        return v * r * gain

    kgain = jnp.concatenate([kgain_ref[...]] * 2, axis=1)
    qgain = jnp.concatenate([qgain_ref[...]] * 2, axis=1)

    def kv_tile(i, carry):
        rows = pl.ds(pl.multiple_of(i * 256, 256), 256)
        kv = jnp.dot(nrm[rows, :], w0[...].reshape(2048, 256), preferred_element_type=F32)
        kb[z, rows, :] = half_norm(kv[:, 0:128], kgain).astype(BF16)
        vb[z, :, rows] = kv[:, 128:256].T.astype(BF16)
        return carry

    def q_tile(i, carry):
        rows = pl.ds(pl.multiple_of(i * 128, 128), 128)
        rows2 = pl.ds(pl.multiple_of(i * 128 + 512, 128), 128)
        q = jnp.dot(
            nrm[rows, :], w1[...].reshape(2048, 128), preferred_element_type=F32
        )
        qt = half_norm(q, qgain).T.astype(BF16)
        qb[0:64, rows] = qt[0:64]
        qb[64:128, rows2] = qt[64:128]
        return carry

    lax.fori_loop(0, 2, kv_tile, 0)

    bufs = (kb, vb)

    def kv_copy(d, w, s):
        i = zz(z - (s - 1)) if d == 0 else zz(z + (s - 1))
        ref = bufs[w].at[i]
        return rc(ref, ref, kvs.at[d, w, s - 1], kvr.at[d, w, s - 1], dev_z[d])

    def kv_wait(d, w, s):
        i = zz(z - s) if d == 0 else zz(z + s)
        ref = bufs[w].at[i]
        rc(ref, ref, kvs.at[d, w, s - 1], kvr.at[d, w, s - 1], dev_z[d]).wait_recv()

    factor = LOG2E * 0.125

    for d in range(2):
        kv_copy(d, 0, 1).start()
    z_serve(5)
    for d in range(2):
        kv_copy(d, 1, 1).start()
    y_relay(1, 4, 5, 6, 7, 8)
    y_relay(4, 2, 3, 4)
    y_send(2, 2, 3)

    def attend(b):
        cols = [slice(i * 256, i * 256 + 256) for i in range(4)]
        st = [jnp.dot(kb[b], qb[:, cs], preferred_element_type=F32) for cs in cols]
        for i, cs in enumerate(cols):
            m_old = m_s[:, cs]
            m_new = jnp.maximum(m_old, jnp.max(st[i], axis=0, keepdims=True))
            p = jnp.exp2((st[i] - m_new) * factor)
            a = jnp.exp2((m_old - m_new) * factor)
            l_s[:, cs] = l_s[:, cs] * a + jnp.sum(p, axis=0, keepdims=True)
            acc_s[:, cs] = acc_s[:, cs] * a + jnp.dot(
                vb[b], p.astype(BF16), preferred_element_type=F32
            )
            m_s[:, cs] = m_new

    def conv_project(half):
        def tile(j, carry):
            i = 3 * j if half == 0 else 1 + j
            rows = pl.ds(pl.multiple_of(i * 128, 128), 128)
            rows8 = pl.ds(pl.multiple_of(i * 128 + 8, 8), 128)
            r = jnp.dot(nrm[rows, :], w2[...].reshape(2048, 768), preferred_element_type=F32)
            postb[rows, :] = r[:, 0:256].astype(BF16)
            signal = (r[:, 256:512] * r[:, 512:768]).astype(BF16)
            sigb[rows, :] = signal
            sigf[rows8, :] = signal.astype(F32)
            return carry

        lax.fori_loop(0, 2, tile, 0)

    def halo_copy(d):
        src = sigb.at[pl.ds(496, 16)] if d == 0 else sigb.at[pl.ds(0, 16)]
        return rc(src, halo.at[d], hs.at[d], hr.at[d], dev_z[d])

    def conv_filter():
        before = halo[0].astype(F32)[8:16]
        after = halo[1].astype(F32)[0:8]
        sigf[0:8, :] = jnp.where(z > 0, before, 0.0)
        sigf[520:528, :] = jnp.where(z < NZ - 1, after, 0.0)
        taps = taps_ref[:, pl.ds(pl.multiple_of(t * 256, 256), 256)]
        for i in range(4):
            r = i * 128
            filtered = (
                taps[0:1] * sigf[r + 7 : r + 135, :]
                + taps[1:2] * sigf[r + 8 : r + 136, :]
                + taps[2:3] * sigf[r + 9 : r + 137, :]
            )
            conv[r : r + 128, :] = (
                postb[r : r + 128, :].astype(F32) * filtered
            ).astype(BF16)

    up, down = pl.ds(0, 32), pl.ds(32, 32)

    def conv_out(q):
        def tile(j, carry):
            k = 4 * q + 2 * j
            w = jnp.concatenate(
                [w3[slab_at(k + i)].reshape(128, 256) for i in range(2)], axis=0
            )
            r = lax.dot_general(
                conv[...], w, (((1,), (1,)), ((), ())), preferred_element_type=F32
            )
            cols = pl.ds(pl.multiple_of(j * 256, 256), 256)
            part[q, :, :, :, cols] = r.astype(BF16).reshape(NX, 2, 64, 256)
            return carry

        lax.fori_loop(0, 2, tile, 0)

    def sums(q, i):
        p, f = psum.at[q], fin.at[q]
        src, dst, dev = (
            (part.at[q, :, 1 - c], pair_in.at[q], dev_c),
            (p.at[far, up], rel.at[q, 0], dev_x[0]),
            (p.at[far, down], rel.at[q, 1], dev_x[1]),
            (p.at[right, down], f.at[0, down], dev_x[0]),
            (p.at[left, up], f.at[1, up], dev_x[1]),
            (p.at[right, up], f.at[0, up], dev_x[0]),
            (p.at[left, down], f.at[1, down], dev_x[1]),
        )[i]
        return rc(src, dst, rs.at[q, i], rr.at[q, i], dev)

    def sum_pair(q, j):
        psum[q, j] = (part[q, j, c].astype(F32) + pair_in[q, j].astype(F32)).astype(BF16)

    def sum_start(q, *steps):
        y_done(3, *steps)
        conv_out(q)
        sums(q, 0).start()

    def sum_first(q):
        sums(q, 0).wait_recv()
        sum_pair(q, far)
        sums(q, 1).start()
        sums(q, 2).start()
        sum_pair(q, right)
        sum_pair(q, left)
        sums(q, 3).start()
        sums(q, 4).start()

    def sum_second(q):
        sums(q, 1).wait_recv()
        psum[q, right, 0:32] = (
            psum[q, right, 0:32].astype(F32) + rel[q, 0].astype(F32)
        ).astype(BF16)
        sums(q, 5).start()
        sums(q, 2).wait_recv()
        psum[q, left, 32:64] = (
            psum[q, left, 32:64].astype(F32) + rel[q, 1].astype(F32)
        ).astype(BF16)
        sums(q, 6).start()

    def sum_last(q):
        for i in (3, 4, 5, 6):
            sums(q, i).wait_recv()
        total = part[q, x, c].astype(F32) + pair_in[q, x].astype(F32)
        total = total + fin[q, 0].astype(F32) + fin[q, 1].astype(F32)
        for i in range(4):
            col = pl.multiple_of(slab_at(4 * q + i) * 128, 128)
            acc_o[:, pl.ds(col, 128)] = total[:, i * 128 : i * 128 + 128]

    def relay(w, s):
        for d in range(2):
            kv_wait(d, w, s)
            if d == w:
                kv_copy(d, w, s + 1).start()
            else:

                @pl.when(s < 7)
                def _():
                    kv_copy(d, w, s + 1).start()

    def halo_send():
        for d in range(2):
            halo_copy(d).start()

    def conv_finish():
        for d in range(2):
            halo_copy(d).wait_recv()
        conv_filter()

    jobs = {
        (1, 0): lambda: (z_serve(6), y_relay(4, 5, 6, 7, 8), y_send(2, 4)),
        (1, 1): lambda: (y_relay(2, 2), y_send(2, 5)),
        (2, 0): lambda: (z_serve(7), y_relay(2, 3), y_send(2, 6), y_done(4, *range(9)), a_begin()),
        (2, 1): lambda: (y_relay(2, 4),),
        (3, 0): lambda: (z_serve(8), y_relay(2, 5), y_send(2, 7)),
        (3, 1): lambda: (y_relay(2, 6), y_send(2, 8), y_send(3, 0, 1)),
        (4, 0): lambda: (y_send(3, 2, 3),),
        (4, 1): lambda: (y_relay(2, 7), y_send(3, 4, 5), a_middle()),
        (5, 0): lambda: (y_relay(2, 8), y_relay(3, 0, 1), y_send(3, 6, 7, 8)),
        (5, 1): lambda: (y_relay(3, 2, 3), y_done(2, *range(9)), conv_project(0), halo_send()),
        (6, 0): lambda: (y_relay(3, 4, 5, 6), conv_project(1), a_late()),
        (6, 1): lambda: (y_relay(3, 7, 8), conv_finish(), sum_start(0, 0, 1, 2), sum_start(1, 3, 4)),
        (7, 0): lambda: (sum_start(2, 5, 6), sum_first(0), sum_first(1)),
        (7, 1): lambda: (sum_start(3, 7, 8), sum_first(2)),
    }

    def serve(s, w):
        for (at, half), job in jobs.items():
            if half == w:

                @pl.when(s == at)
                def _(job=job):
                    job()

    relay(0, 1)
    jobs[1, 0]()
    relay(1, 1)
    jobs[1, 1]()
    y_done(1, *range(9))
    lax.fori_loop(0, 4, q_tile, 0)
    attend(z)

    def kv_step(s, carry):
        relay(0, s)
        serve(s, 0)
        attend(zz(z - (s - 1)))
        relay(1, s)
        serve(s, 1)
        attend(zz(z + (s - 1)))
        return carry

    lax.fori_loop(2, 8, kv_step, 0)
    sum_first(3)
    attend(zz(z - 7))
    sum_second(0)
    sum_second(1)
    attend(zz(z + 7))
    sum_second(2)
    kv_wait(0, 0, 8)
    kv_wait(1, 1, 8)
    attend(zz(z + 8))

    lane = lax.broadcasted_iota(jnp.int32, (1, 8), 1)
    lam = jnp.sum(jnp.where(lane == t, lam_ref[...], 0.0), axis=1, keepdims=True)
    inv = 1.0 / l_s[...]
    head = acc_s[:, 0:512] * inv[:, 0:512] - lam * (acc_s[:, 512:1024] * inv[:, 512:1024])
    r = lax.rsqrt(jnp.sum(head * head, axis=0, keepdims=True) * (1.0 / 128) + EPS)
    hid[...] = ((head * r).T * hgain_ref[...]).astype(BF16)

    def give(i):
        peer = (t + i) % 8
        rows = pl.ds(pl.multiple_of(peer * 64, 64), 64)
        return rc(hid.at[rows], ah.at[t], als.at[i - 1], alr.at[i - 1], {"tp": peer})

    for i in range(1, 8):
        give(i).start()
    ah[t] = hid[pl.ds(pl.multiple_of(t * 64, 64), 64), :]
    sum_second(3)
    a_finish()
    for q in range(4):
        sum_last(q)
    for i in range(1, 8):
        source = (t + 8 - i) % 8
        rc(ah.at[source], ah.at[source], als.at[i - 1], alr.at[i - 1], dev_c).wait_recv()
    whole = jnp.concatenate([ah[i] for i in range(8)], axis=1)
    for n in range(8):
        w = jnp.concatenate(
            [wa[i, 2 * n : 2 * n + 2].reshape(256, 128) for i in range(8)], axis=1
        )
        r = lax.dot_general(whole, w, (((1,), (1,)), ((), ())), preferred_element_type=F32)
        cols = slice(n * 256, n * 256 + 256)
        out_ref[:, cols] = (acc_o[:, cols] + r).astype(BF16)

    for g in range(5):
        for d in range(2):
            for step in range(1, zsteps[g][d] + 1):
                z_copy(g, d, step, 2 if g in (0, 1, 4) and step > 1 else 1).wait_send()

    def y_drain(k, carry):
        for g in range(5):
            for d in range(2):
                y_direct(g, k, d, True).wait_send()
                if g > 0:
                    y_half(g, k, d, True).wait_send()
        return carry

    lax.fori_loop(0, 16, y_drain, 0)

    def y_drain_0(k, carry):
        for d in range(2):
            y_half(0, k, d, True).wait_send()
        return carry

    lax.fori_loop(0, 13, y_drain_0, 0)
    for k in far_slabs:
        y_far(0, k, True).wait_send()
    for w in range(2):
        for d in range(2):
            for s in range(1, 9 if d == w else 8):
                kv_copy(d, w, s).wait_send()
    x_drain()
    a_drain()
    for d in range(2):
        halo_copy(d).wait_send()
    for q in range(4):
        for i in range(7):
            sums(q, i).wait_send()
    for i in range(1, 8):
        give(i).wait_send()


def per_device(
    inputs, norm_gain, query_weight, key_weight, value_weight, query_gain, key_gain,
    mix_lambda, head_gain, post_gate_weight, pre_gate_weight, inner_weight, conv_taps,
    attn_out_weight, conv_out_weight,
):
    hbm = pl.BlockSpec(memory_space=pl.ANY)
    vmem = pl.BlockSpec(memory_space=pltpu.VMEM)
    sem = pltpu.SemaphoreType.DMA
    out = pl.pallas_call(
        body,
        out_shape=jax.ShapeDtypeStruct((64, 2048), BF16),
        in_specs=[hbm] * 15,
        out_specs=vmem,
        scratch_shapes=[
            pltpu.VMEM((1, 2048), F32),
            pltpu.VMEM((1, 64), F32),
            pltpu.VMEM((1, 64), F32),
            pltpu.VMEM((1, 128), F32),
            pltpu.VMEM((3, 2048), F32),
            pltpu.VMEM((1, 8), F32),
            pltpu.VMEM((8, 512, 256), BF16),
            pltpu.VMEM((512, 2048), BF16),
            pltpu.VMEM((NZ, NY, 32, 256), BF16),
            pltpu.VMEM((NZ, NY, 32, 128), BF16),
            pltpu.VMEM((8, NZ, NY, 32, 128), BF16),
            pltpu.VMEM((NZ, NY, 32, 768), BF16),
            pltpu.VMEM((NZ, NY, 32, 256), BF16),
            pltpu.VMEM((NZ, 512, 128), BF16),
            pltpu.VMEM((NZ, 128, 512), BF16),
            pltpu.VMEM((128, 1024), BF16),
            pltpu.VMEM((1, 1024), F32),
            pltpu.VMEM((1, 1024), F32),
            pltpu.VMEM((128, 1024), F32),
            pltpu.VMEM((512, 128), BF16),
            pltpu.VMEM((8, 64, 128), BF16),
            pltpu.VMEM((512, 256), BF16),
            pltpu.VMEM((512, 256), BF16),
            pltpu.VMEM((528, 256), F32),
            pltpu.VMEM((2, 16, 256), BF16),
            pltpu.VMEM((512, 256), BF16),
            pltpu.VMEM((4, NX, 2, 64, 512), BF16),
            pltpu.VMEM((4, NX, 64, 512), BF16),
            pltpu.VMEM((4, NX, 64, 512), BF16),
            pltpu.VMEM((4, 2, 32, 512), BF16),
            pltpu.VMEM((4, 2, 64, 512), BF16),
            pltpu.VMEM((64, 2048), F32),
            sem((15,)),
            sem((9,)),
            sem((9,)),
            sem((9,)),
            sem((9,)),
            sem((5, 2, 8)),
            sem((5, 2, 8)),
            sem((5, 2, 16)),
            sem((5, 2, 16)),
            sem((5, 2, 16)),
            sem((5, 2, 16)),
            sem((2, 2, 8)),
            sem((2, 2, 8)),
            sem((2,)),
            sem((2,)),
            sem((4, 7)),
            sem((4, 7)),
            sem((7,)),
            sem((7,)),
        ],
        compiler_params=pltpu.CompilerParams(
            collective_id=0, has_side_effects=True, vmem_limit_bytes=60 * 1024 * 1024,
        ),
    )(
        inputs[0], query_weight, key_weight, value_weight, post_gate_weight,
        pre_gate_weight, inner_weight, attn_out_weight, conv_out_weight,
        norm_gain.reshape(1, -1),
        query_gain.reshape(1, -1),
        key_gain.reshape(1, -1),
        head_gain.reshape(1, -1),
        conv_taps,
        mix_lambda.reshape(1, -1),
    )
    return out[None]


def solution(mesh):
    rows = P(("sp", "fs"), "tp")
    placed = (
        P("fs", "sp", "tp"), P(), rows, rows, rows, P(), P(), P(), P(),
        rows, rows, rows, P(), rows, rows,
    )
    return jax.shard_map(
        per_device,
        mesh=mesh,
        in_specs=placed,
        out_specs=P("fs", ("sp", "tp"), None),
        check_vma=False,
    )
```

```python
import functools

import jax
import jax.numpy as jnp
from jax import lax
from jax.experimental import pallas as pl
from jax.experimental.pallas import tpu as pltpu
from jax.sharding import PartitionSpec as P

EPS = 1e-06
MESH = pl.DeviceIdType.MESH
F32 = jnp.float32
BF16 = jnp.bfloat16
LOG2E = 1.4426950408889634

NZ, NY, NX = 16, 4, 4


def body(
    tok_ref, wq_ref, wk_ref, wv_ref, wpost_ref, wpre_ref, winner_ref, wao_ref, wco_ref,
    ngain_hbm, qgain_hbm, kgain_hbm, hgain_hbm, taps_hbm, lam_hbm,
    out_ref,
    ngain_ref, qgain_ref, kgain_ref, hgain_ref, taps_ref, lam_ref,
    xg, nrm, w0, w1, wa, w2, w3, kb, vb, qb, m_s, l_s, acc_s, hid, ah, conv, sigb, sigf, halo, postb,
    part, pair_in, psum, rel, fin, acc_o,
    lsem, xss, xrs, xas, xar, zss, zrs, yds, ydr, yfs, yfr,
    kvs, kvr, hs, hr, rs, rr, als, alr,
):
    z = lax.axis_index("sp")
    y = lax.axis_index("fs")
    t = lax.axis_index("tp")
    x = t // 2
    c = t % 2

    def zz(i):
        return (i + 2 * NZ) % NZ

    def yy(i):
        return (i + 2 * NY) % NY

    def xx(i):
        return (i + 2 * NX) % NX

    dev_z = ({"sp": zz(z + 1)}, {"sp": zz(z - 1)})
    dev_zz = ({"sp": zz(z + 2)}, {"sp": zz(z - 2)})
    dev_y = ({"fs": yy(y + 1)}, {"fs": yy(y - 1)})
    dev_x = ({"tp": xx(x + 1) * 2 + c}, {"tp": xx(x - 1) * 2 + c})
    other = x * 2 + (1 - c)
    dev_c = {"tp": other}
    group = tuple({"tp": (t + i) % 8} for i in range(1, 8))
    dev_far = {"fs": yy(y + 2)}
    peers = dev_z + dev_zz + dev_y + (dev_far,) + group

    def rc(src, dst, ssem, rsem, dev):
        return pltpu.make_async_remote_copy(
            src_ref=src, dst_ref=dst, send_sem=ssem, recv_sem=rsem,
            device_id=dev, device_id_type=MESH,
        )

    own = (
        (tok_ref, xg.at[t]),
        (wk_ref, w0.at[z, y, :, 0:128]),
        (wv_ref, w0.at[z, y, :, 128:256]),
        (wq_ref, w1.at[z, y]),
        (wao_ref, wa.at[t, z, y]),
        (wpost_ref, w2.at[z, y, :, 0:256]),
        (wpre_ref, w2.at[z, y, :, 256:512]),
        (winner_ref, w2.at[z, y, :, 512:768]),
        (wco_ref, w3.at[z, y]),
        (ngain_hbm, ngain_ref),
        (qgain_hbm, qgain_ref),
        (kgain_hbm, kgain_ref),
        (hgain_hbm, hgain_ref),
        (taps_hbm, taps_ref),
        (lam_hbm, lam_ref),
    )
    local = [pltpu.make_async_copy(s, d, lsem.at[i]) for i, (s, d) in enumerate(own)]
    for cp in local:
        cp.start()
    barrier = pltpu.get_barrier_semaphore()
    for dev in peers:
        pl.semaphore_signal(barrier, inc=1, device_id=dev, device_id_type=MESH)

    qb[...] = jnp.zeros_like(qb)
    m_s[...] = jnp.full_like(m_s, -1e30)
    l_s[...] = jnp.zeros_like(l_s)
    acc_s[...] = jnp.zeros_like(acc_s)

    pl.semaphore_wait(barrier, len(peers))

    own_wa = wa.at[t]
    ws = (w0, w1, w2, w3, own_wa)
    zsteps = ((7, 8), (8, 7), (7, 8), (8, 7), (8, 7))

    def z_slab(d, s):
        return zz(z - s) if d == 0 else zz(z + s)

    def z_copy(g, d, s, stride=1):
        ref = ws[g].at[z_slab(d, s - stride), y]
        dev = (dev_z if stride == 1 else dev_zz)[d]
        return rc(ref, ref, zss.at[g, d, s - 1], zrs.at[g, d, s - 1], dev)

    def z_wait(g, d, s):
        ref = ws[g].at[z_slab(d, s), y]
        rc(ref, ref, zss.at[g, d, s - 1], zrs.at[g, d, s - 1], dev_z[d]).wait_recv()

    def z_serve(s):
        for g in (2, 3):
            for d in range(2):
                if s <= zsteps[g][d]:
                    z_wait(g, d, s)
                    if s < zsteps[g][d]:
                        z_copy(g, d, s + 1).start()

    def level(s):
        return (0,) if s == 0 else (15,) if s == 8 else (2 * s - 1, 2 * s)

    def slab_at(k):
        return zz(z + (k + 1) // 2 * (1 - 2 * (k % 2)))

    def y_direct(g, k, d, mine):
        col = y if mine else yy(y - 1) if d == 0 else yy(y + 1)
        ref = ws[g].at[slab_at(k), col]
        return rc(ref, ref, yds.at[g, d, k], ydr.at[g, d, k], dev_y[d])

    def y_half(g, k, d, mine):
        col = yy(y + 2) if not mine else yy(y - 1) if d == 0 else yy(y + 1)
        ref = ws[g].at[slab_at(k), col, pl.ds(16 * d, 16)]
        return rc(ref, ref, yfs.at[g, d, k], yfr.at[g, d, k], dev_y[d])

    def y_send(g, *steps):
        for s in steps:
            for k in level(s):
                for d in range(2):
                    y_direct(g, k, d, True).start()

    def y_relay(g, *steps):
        for s in steps:
            for k in level(s):
                for d in range(2):
                    y_direct(g, k, d, False).wait_recv()
                    y_half(g, k, d, True).start()

    def y_far(g, k, mine):
        ref = ws[g].at[slab_at(k), y if mine else yy(y + 2)]
        return rc(ref, ref, yfs.at[g, 0, k], yfr.at[g, 0, k], dev_far)

    def y_done(g, *steps):
        for s in steps:
            for k in level(s):
                for d in range(2):
                    y_half(g, k, d, False).wait_recv()

    left, right, far = xx(x - 1), xx(x + 1), xx(x + 2)

    def x_gather(buf, lo, hi, ss, sr, start):
        def send(k, slot, dev, piece=None):
            ref = buf.at[slot] if piece is None else buf.at[slot, piece]
            start(rc(ref, ref, ss.at[k], sr.at[k], dev))

        def wait(k, slot, piece=None):
            ref = buf.at[slot] if piece is None else buf.at[slot, piece]
            rc(ref, ref, ss.at[k], sr.at[k], dev_c).wait_recv()

        def begin():
            send(0, t, dev_x[0])
            send(1, t, dev_x[1])
            send(2, t, dev_c)

        def middle():
            wait(0, left * 2 + c)
            send(5, left * 2 + c, dev_x[0], lo)
            wait(1, right * 2 + c)
            send(6, right * 2 + c, dev_x[1], hi)
            send(3, left * 2 + c, dev_c)
            send(4, right * 2 + c, dev_c)

        def late():
            wait(5, far * 2 + c, lo)
            send(7, far * 2 + c, dev_c, lo)
            wait(6, far * 2 + c, hi)
            send(8, far * 2 + c, dev_c, hi)

        def finish():
            wait(2, other)
            wait(3, left * 2 + (1 - c))
            wait(4, right * 2 + (1 - c))
            wait(7, far * 2 + (1 - c), lo)
            wait(8, far * 2 + (1 - c), hi)

        def drain():
            for k, slot, piece in (
                (0, t, None), (1, t, None), (2, t, None),
                (5, left * 2 + c, lo), (6, right * 2 + c, hi),
                (3, left * 2 + c, None), (4, right * 2 + c, None),
                (7, far * 2 + c, lo), (8, far * 2 + c, hi),
            ):
                ref = buf.at[slot] if piece is None else buf.at[slot, piece]
                rc(ref, ref, ss.at[k], sr.at[k], dev_c).wait_send()

        return begin, middle, late, finish, drain

    x_begin, x_service_a, x_service_b, x_finish, x_drain = x_gather(
        xg, pl.ds(0, 256), pl.ds(256, 256), xss, xrs, lambda copy: copy.start()
    )
    a_begin, a_middle, a_late, a_finish, a_drain = x_gather(
        wa, pl.ds(0, 8), pl.ds(8, 8), xas, xar, lambda copy: copy.start()
    )

    for i in (1, 2):
        local[i].wait()
    for stride in (1, 2):
        for d in range(2):
            z_copy(0, d, stride, stride).start()
    local[0].wait()
    x_begin()
    y_send(0, 0)
    local[3].wait()
    for stride in (1, 2):
        for d in range(2):
            z_copy(1, d, stride, stride).start()
    for i in range(4, 9):
        local[i].wait()
    for stride in (1, 2):
        for d in range(2):
            z_copy(4, d, stride, stride).start()
    for g in (2, 3):
        for d in range(2):
            z_copy(g, d, 1).start()
    for i in range(9, len(local)):
        local[i].wait()

    def normalize():
        def tile(i, carry):
            rows = pl.ds(pl.multiple_of(i * 32, 32), 32)
            total = jnp.zeros((32, 256), F32)
            for b in range(8):
                v = xg[b, rows, :].astype(F32)
                total = total + v * v
            r = lax.rsqrt(jnp.sum(total, axis=-1, keepdims=True) * (1.0 / 2048) + EPS)
            for b in range(8):
                v = xg[b, rows, :].astype(F32) * r * ngain_ref[:, b * 256 : (b + 1) * 256]
                nrm[rows, b * 256 : (b + 1) * 256] = v.astype(BF16)
            return carry

        lax.fori_loop(0, 16, tile, 0)

    def z_strides(g, r):
        for s in (2 * r - 1, 2 * r):
            for d in range(2):
                if s <= zsteps[g][d]:
                    z_wait(g, d, s)
                    if s + 2 <= zsteps[g][d]:
                        z_copy(g, d, s + 2, 2).start()

    def z_round(r):
        z_strides(0, r)
        y_send(0, 2 * r - 1, 2 * r)
        if r > 1:
            z_strides(1, r - 1)
        if r > 2:
            z_strides(4, r - 2)

    far_slabs = level(7) + level(8)

    z_round(1)
    y_relay(0, 0)
    y_send(1, 0)
    y_send(2, 0)
    z_serve(1)
    z_round(2)
    x_service_a()
    y_relay(0, 1, 2)
    y_send(1, 1, 2)
    y_send(2, 1)
    z_serve(2)
    z_round(3)
    y_relay(0, 3, 4)
    y_relay(1, 0)
    y_send(1, 3)
    z_serve(3)
    x_service_b()
    z_round(4)
    for k in far_slabs:
        y_far(0, k, True).start()
    y_relay(0, 5, 6)
    y_send(1, 4, 5, 6)
    y_relay(2, 0)
    y_send(4, 0, 1, 2, 3, 4)
    z_serve(4)
    x_finish()
    normalize()
    z_strides(1, 4)
    z_strides(4, 3)
    y_send(1, 7, 8)
    y_send(4, 5, 6)
    y_done(0, *range(7))
    for k in far_slabs:
        y_far(0, k, False).wait_recv()
        for d in range(2):
            y_direct(0, k, d, False).wait_recv()

    def half_norm(v, gain):
        first = lax.broadcasted_iota(jnp.int32, v.shape, 1) < 64
        sq = v * v
        s1 = jnp.sum(jnp.where(first, sq, 0.0), axis=-1, keepdims=True)
        s2 = jnp.sum(jnp.where(first, 0.0, sq), axis=-1, keepdims=True)
        r = jnp.where(
            first, lax.rsqrt(s1 * (1.0 / 64) + EPS), lax.rsqrt(s2 * (1.0 / 64) + EPS)
        )
        return v * r * gain

    kgain = jnp.concatenate([kgain_ref[...]] * 2, axis=1)
    qgain = jnp.concatenate([qgain_ref[...]] * 2, axis=1)

    def kv_tile(i, carry):
        rows = pl.ds(pl.multiple_of(i * 256, 256), 256)
        kv = jnp.dot(nrm[rows, :], w0[...].reshape(2048, 256), preferred_element_type=F32)
        kb[z, rows, :] = half_norm(kv[:, 0:128], kgain).astype(BF16)
        vb[z, :, rows] = kv[:, 128:256].T.astype(BF16)
        return carry

    def q_tile(i, carry):
        rows = pl.ds(pl.multiple_of(i * 128, 128), 128)
        rows2 = pl.ds(pl.multiple_of(i * 128 + 512, 128), 128)
        q = jnp.dot(
            nrm[rows, :], w1[...].reshape(2048, 128), preferred_element_type=F32
        )
        qt = half_norm(q, qgain).T.astype(BF16)
        qb[0:64, rows] = qt[0:64]
        qb[64:128, rows2] = qt[64:128]
        return carry

    lax.fori_loop(0, 2, kv_tile, 0)

    bufs = (kb, vb)

    def kv_copy(d, w, s):
        i = zz(z - (s - 1)) if d == 0 else zz(z + (s - 1))
        ref = bufs[w].at[i]
        return rc(ref, ref, kvs.at[d, w, s - 1], kvr.at[d, w, s - 1], dev_z[d])

    def kv_wait(d, w, s):
        i = zz(z - s) if d == 0 else zz(z + s)
        ref = bufs[w].at[i]
        rc(ref, ref, kvs.at[d, w, s - 1], kvr.at[d, w, s - 1], dev_z[d]).wait_recv()

    factor = LOG2E * 0.125

    for d in range(2):
        kv_copy(d, 0, 1).start()
    z_serve(5)
    for d in range(2):
        kv_copy(d, 1, 1).start()
    y_relay(1, 1, 2, 3, 4)
    y_relay(2, 1)
    y_relay(4, 0, 1)
    z_strides(4, 4)
    y_send(4, 7, 8)
    y_send(2, 2, 3)
    y_relay(1, 5, 6, 7, 8)
    y_relay(4, 2, 3, 4)

    def attend(b):
        cols = [slice(i * 256, i * 256 + 256) for i in range(4)]
        st = [jnp.dot(kb[b], qb[:, cs], preferred_element_type=F32) for cs in cols]
        for i, cs in enumerate(cols):
            m_old = m_s[:, cs]
            m_new = jnp.maximum(m_old, jnp.max(st[i], axis=0, keepdims=True))
            p = jnp.exp2((st[i] - m_new) * factor)
            a = jnp.exp2((m_old - m_new) * factor)
            l_s[:, cs] = l_s[:, cs] * a + jnp.sum(p, axis=0, keepdims=True)
            acc_s[:, cs] = acc_s[:, cs] * a + jnp.dot(
                vb[b], p.astype(BF16), preferred_element_type=F32
            )
            m_s[:, cs] = m_new

    def conv_project(half):
        def tile(j, carry):
            i = 3 * j if half == 0 else 1 + j
            rows = pl.ds(pl.multiple_of(i * 128, 128), 128)
            rows8 = pl.ds(pl.multiple_of(i * 128 + 8, 8), 128)
            r = jnp.dot(nrm[rows, :], w2[...].reshape(2048, 768), preferred_element_type=F32)
            postb[rows, :] = r[:, 0:256].astype(BF16)
            signal = (r[:, 256:512] * r[:, 512:768]).astype(BF16)
            sigb[rows, :] = signal
            sigf[rows8, :] = signal.astype(F32)
            return carry

        lax.fori_loop(0, 2, tile, 0)

    def halo_copy(d):
        src = sigb.at[pl.ds(496, 16)] if d == 0 else sigb.at[pl.ds(0, 16)]
        return rc(src, halo.at[d], hs.at[d], hr.at[d], dev_z[d])

    def conv_filter():
        before = halo[0].astype(F32)[8:16]
        after = halo[1].astype(F32)[0:8]
        sigf[0:8, :] = jnp.where(z > 0, before, 0.0)
        sigf[520:528, :] = jnp.where(z < NZ - 1, after, 0.0)
        taps = taps_ref[:, pl.ds(pl.multiple_of(t * 256, 256), 256)]
        for i in range(4):
            r = i * 128
            filtered = (
                taps[0:1] * sigf[r + 7 : r + 135, :]
                + taps[1:2] * sigf[r + 8 : r + 136, :]
                + taps[2:3] * sigf[r + 9 : r + 137, :]
            )
            conv[r : r + 128, :] = (
                postb[r : r + 128, :].astype(F32) * filtered
            ).astype(BF16)

    up, down = pl.ds(0, 32), pl.ds(32, 32)

    def conv_out(q):
        def tile(j, carry):
            k = 4 * q + 2 * j
            w = jnp.concatenate(
                [w3[slab_at(k + i)].reshape(128, 256) for i in range(2)], axis=0
            )
            r = lax.dot_general(
                conv[...], w, (((1,), (1,)), ((), ())), preferred_element_type=F32
            )
            cols = pl.ds(pl.multiple_of(j * 256, 256), 256)
            part[q, :, :, :, cols] = r.astype(BF16).reshape(NX, 2, 64, 256)
            return carry

        lax.fori_loop(0, 2, tile, 0)

    def sums(q, i):
        p, f = psum.at[q], fin.at[q]
        src, dst, dev = (
            (part.at[q, :, 1 - c], pair_in.at[q], dev_c),
            (p.at[far, up], rel.at[q, 0], dev_x[0]),
            (p.at[far, down], rel.at[q, 1], dev_x[1]),
            (p.at[right, down], f.at[0, down], dev_x[0]),
            (p.at[left, up], f.at[1, up], dev_x[1]),
            (p.at[right, up], f.at[0, up], dev_x[0]),
            (p.at[left, down], f.at[1, down], dev_x[1]),
        )[i]
        return rc(src, dst, rs.at[q, i], rr.at[q, i], dev)

    def sum_pair(q, j):
        psum[q, j] = (part[q, j, c].astype(F32) + pair_in[q, j].astype(F32)).astype(BF16)

    def sum_start(q, *steps):
        y_done(3, *steps)
        conv_out(q)
        sums(q, 0).start()

    def sum_first(q):
        sums(q, 0).wait_recv()
        sum_pair(q, far)
        sums(q, 1).start()
        sums(q, 2).start()
        sum_pair(q, right)
        sum_pair(q, left)
        sums(q, 3).start()
        sums(q, 4).start()

    def sum_second(q):
        sums(q, 1).wait_recv()
        psum[q, right, 0:32] = (
            psum[q, right, 0:32].astype(F32) + rel[q, 0].astype(F32)
        ).astype(BF16)
        sums(q, 5).start()
        sums(q, 2).wait_recv()
        psum[q, left, 32:64] = (
            psum[q, left, 32:64].astype(F32) + rel[q, 1].astype(F32)
        ).astype(BF16)
        sums(q, 6).start()

    def sum_last(q):
        for i in (3, 4, 5, 6):
            sums(q, i).wait_recv()
        total = part[q, x, c].astype(F32) + pair_in[q, x].astype(F32)
        total = total + fin[q, 0].astype(F32) + fin[q, 1].astype(F32)
        for i in range(4):
            col = pl.multiple_of(slab_at(4 * q + i) * 128, 128)
            acc_o[:, pl.ds(col, 128)] = total[:, i * 128 : i * 128 + 128]

    def relay(w, s):
        for d in range(2):
            kv_wait(d, w, s)
            if d == w:
                kv_copy(d, w, s + 1).start()
            else:

                @pl.when(s < 7)
                def _():
                    kv_copy(d, w, s + 1).start()

    def halo_send():
        for d in range(2):
            halo_copy(d).start()

    def conv_finish():
        for d in range(2):
            halo_copy(d).wait_recv()
        conv_filter()

    jobs = {
        (1, 0): lambda: (z_serve(6), y_relay(4, 5, 6), y_send(2, 4)),
        (1, 1): lambda: (y_relay(4, 7, 8), y_relay(2, 2), y_send(2, 5)),
        (2, 0): lambda: (z_serve(7), y_relay(2, 3), y_send(2, 6)),
        (2, 1): lambda: (y_relay(2, 4), y_send(2, 7), y_done(4, *range(9)), a_begin()),
        (3, 0): lambda: (z_serve(8), y_relay(2, 5), y_send(2, 8)),
        (3, 1): lambda: (y_relay(2, 6),),
        (4, 0): lambda: (y_relay(2, 7), y_send(3, 0, 1)),
        (4, 1): lambda: (y_relay(2, 8), y_send(3, 2, 3, 4, 5, 6, 7, 8)),
        (5, 0): lambda: (y_relay(3, 0, 1), y_done(2, *range(9)), conv_project(0), halo_send()),
        (5, 1): lambda: (y_relay(3, 2, 3, 4, 5), conv_project(1), a_middle()),
        (6, 0): lambda: (y_relay(3, 6, 7, 8), conv_finish(), sum_start(0, 0, 1, 2)),
        (6, 1): lambda: (sum_start(1, 3, 4), sum_start(2, 5, 6), sum_first(0), a_late()),
        (7, 0): lambda: (sum_start(3, 7, 8), sum_first(1), sum_first(2)),
        (7, 1): lambda: (sum_first(3), sum_second(0)),
    }

    def serve(s, w):
        for (at, half), job in jobs.items():
            if half == w:

                @pl.when(s == at)
                def _(job=job):
                    job()

    relay(0, 1)
    jobs[1, 0]()
    relay(1, 1)
    jobs[1, 1]()
    y_done(1, *range(9))
    lax.fori_loop(0, 4, q_tile, 0)
    attend(z)

    def kv_step(s, carry):
        relay(0, s)
        serve(s, 0)
        attend(zz(z - (s - 1)))
        relay(1, s)
        serve(s, 1)
        attend(zz(z + (s - 1)))
        return carry

    lax.fori_loop(2, 8, kv_step, 0)
    attend(zz(z - 7))
    sum_second(1)
    sum_second(2)
    attend(zz(z + 7))
    sum_second(3)
    kv_wait(0, 0, 8)
    kv_wait(1, 1, 8)
    attend(zz(z + 8))

    lane = lax.broadcasted_iota(jnp.int32, (1, 8), 1)
    lam = jnp.sum(jnp.where(lane == t, lam_ref[...], 0.0), axis=1, keepdims=True)
    inv = 1.0 / l_s[...]
    head = acc_s[:, 0:512] * inv[:, 0:512] - lam * (acc_s[:, 512:1024] * inv[:, 512:1024])
    r = lax.rsqrt(jnp.sum(head * head, axis=0, keepdims=True) * (1.0 / 128) + EPS)
    hid[...] = ((head * r).T * hgain_ref[...]).astype(BF16)

    def give(i):
        peer = (t + i) % 8
        rows = pl.ds(pl.multiple_of(peer * 64, 64), 64)
        return rc(hid.at[rows], ah.at[t], als.at[i - 1], alr.at[i - 1], {"tp": peer})

    for i in range(1, 8):
        give(i).start()
    ah[t] = hid[pl.ds(pl.multiple_of(t * 64, 64), 64), :]
    a_finish()
    for q in range(4):
        sum_last(q)
    def out_part(chip, last):
        rows = jnp.concatenate([ah[2 * chip], ah[2 * chip + 1]], axis=1)
        for n in range(8):
            w = jnp.concatenate(
                [wa[2 * chip + i, 2 * n : 2 * n + 2].reshape(256, 128) for i in range(2)], axis=1
            )
            r = lax.dot_general(rows, w, (((1,), (1,)), ((), ())), preferred_element_type=F32)
            cols = slice(n * 256, n * 256 + 256)
            if last:
                out_ref[:, cols] = (acc_o[:, cols] + r).astype(BF16)
            else:
                acc_o[:, cols] = acc_o[:, cols] + r

    def ah_pair(hop):
        for core in range(2):
            source = xx(x + hop) * 2 + core
            slot = (t - source + 8) % 8 - 1
            rc(ah.at[source], ah.at[source], als.at[slot], alr.at[slot], dev_c).wait_recv()

    own_slot = (t - other + 8) % 8 - 1
    rc(ah.at[other], ah.at[other], als.at[own_slot], alr.at[own_slot], dev_c).wait_recv()
    out_part(x, False)
    ah_pair(1)
    out_part(right, False)
    ah_pair(-1)
    out_part(left, False)
    ah_pair(2)
    out_part(far, True)

    for g in range(5):
        for d in range(2):
            for step in range(1, zsteps[g][d] + 1):
                z_copy(g, d, step, 2 if g in (0, 1, 4) and step > 1 else 1).wait_send()

    def y_drain(k, carry):
        for g in range(5):
            for d in range(2):
                y_direct(g, k, d, True).wait_send()
                if g > 0:
                    y_half(g, k, d, True).wait_send()
        return carry

    lax.fori_loop(0, 16, y_drain, 0)

    def y_drain_0(k, carry):
        for d in range(2):
            y_half(0, k, d, True).wait_send()
        return carry

    lax.fori_loop(0, 13, y_drain_0, 0)
    for k in far_slabs:
        y_far(0, k, True).wait_send()
    for w in range(2):
        for d in range(2):
            for s in range(1, 9 if d == w else 8):
                kv_copy(d, w, s).wait_send()
    x_drain()
    a_drain()
    for d in range(2):
        halo_copy(d).wait_send()
    for q in range(4):
        for i in range(7):
            sums(q, i).wait_send()
    for i in range(1, 8):
        give(i).wait_send()


def per_device(
    inputs, norm_gain, query_weight, key_weight, value_weight, query_gain, key_gain,
    mix_lambda, head_gain, post_gate_weight, pre_gate_weight, inner_weight, conv_taps,
    attn_out_weight, conv_out_weight,
):
    hbm = pl.BlockSpec(memory_space=pl.ANY)
    vmem = pl.BlockSpec(memory_space=pltpu.VMEM)
    sem = pltpu.SemaphoreType.DMA
    out = pl.pallas_call(
        body,
        out_shape=jax.ShapeDtypeStruct((64, 2048), BF16),
        in_specs=[hbm] * 15,
        out_specs=vmem,
        scratch_shapes=[
            pltpu.VMEM((1, 2048), F32),
            pltpu.VMEM((1, 64), F32),
            pltpu.VMEM((1, 64), F32),
            pltpu.VMEM((1, 128), F32),
            pltpu.VMEM((3, 2048), F32),
            pltpu.VMEM((1, 8), F32),
            pltpu.VMEM((8, 512, 256), BF16),
            pltpu.VMEM((512, 2048), BF16),
            pltpu.VMEM((NZ, NY, 32, 256), BF16),
            pltpu.VMEM((NZ, NY, 32, 128), BF16),
            pltpu.VMEM((8, NZ, NY, 32, 128), BF16),
            pltpu.VMEM((NZ, NY, 32, 768), BF16),
            pltpu.VMEM((NZ, NY, 32, 256), BF16),
            pltpu.VMEM((NZ, 512, 128), BF16),
            pltpu.VMEM((NZ, 128, 512), BF16),
            pltpu.VMEM((128, 1024), BF16),
            pltpu.VMEM((1, 1024), F32),
            pltpu.VMEM((1, 1024), F32),
            pltpu.VMEM((128, 1024), F32),
            pltpu.VMEM((512, 128), BF16),
            pltpu.VMEM((8, 64, 128), BF16),
            pltpu.VMEM((512, 256), BF16),
            pltpu.VMEM((512, 256), BF16),
            pltpu.VMEM((528, 256), F32),
            pltpu.VMEM((2, 16, 256), BF16),
            pltpu.VMEM((512, 256), BF16),
            pltpu.VMEM((4, NX, 2, 64, 512), BF16),
            pltpu.VMEM((4, NX, 64, 512), BF16),
            pltpu.VMEM((4, NX, 64, 512), BF16),
            pltpu.VMEM((4, 2, 32, 512), BF16),
            pltpu.VMEM((4, 2, 64, 512), BF16),
            pltpu.VMEM((64, 2048), F32),
            sem((15,)),
            sem((9,)),
            sem((9,)),
            sem((9,)),
            sem((9,)),
            sem((5, 2, 8)),
            sem((5, 2, 8)),
            sem((5, 2, 16)),
            sem((5, 2, 16)),
            sem((5, 2, 16)),
            sem((5, 2, 16)),
            sem((2, 2, 8)),
            sem((2, 2, 8)),
            sem((2,)),
            sem((2,)),
            sem((4, 7)),
            sem((4, 7)),
            sem((7,)),
            sem((7,)),
        ],
        compiler_params=pltpu.CompilerParams(
            collective_id=0, has_side_effects=True, vmem_limit_bytes=60 * 1024 * 1024,
        ),
    )(
        inputs[0], query_weight, key_weight, value_weight, post_gate_weight,
        pre_gate_weight, inner_weight, attn_out_weight, conv_out_weight,
        norm_gain.reshape(1, -1),
        query_gain.reshape(1, -1),
        key_gain.reshape(1, -1),
        head_gain.reshape(1, -1),
        conv_taps,
        mix_lambda.reshape(1, -1),
    )
    return out[None]


def solution(mesh):
    rows = P(("sp", "fs"), "tp")
    placed = (
        P("fs", "sp", "tp"), P(), rows, rows, rows, P(), P(), P(), P(),
        rows, rows, rows, P(), rows, rows,
    )
    return jax.shard_map(
        per_device,
        mesh=mesh,
        in_specs=placed,
        out_specs=P("fs", ("sp", "tp"), None),
        check_vma=False,
    )
```

```python
import functools

import jax
import jax.numpy as jnp
from jax import lax
from jax.experimental import pallas as pl
from jax.experimental.pallas import tpu as pltpu
from jax.sharding import PartitionSpec as P

EPS = 1e-06
MESH = pl.DeviceIdType.MESH
F32 = jnp.float32
BF16 = jnp.bfloat16
LOG2E = 1.4426950408889634

NZ, NY, NX = 16, 4, 4


def body(
    tok_ref, wq_ref, wk_ref, wv_ref, wpost_ref, wpre_ref, winner_ref, wao_ref, wco_ref,
    ngain_hbm, qgain_hbm, kgain_hbm, hgain_hbm, taps_hbm, lam_hbm,
    out_ref,
    ngain_ref, qgain_ref, kgain_ref, hgain_ref, taps_ref, lam_ref,
    xg, nrm, w0, w1, wa, w2, w3, kb, vb, qb, m_s, l_s, acc_s, hid, ah, conv, sigb, sigf, halo, postb,
    part, pair_in, psum, rel, fin, acc_o,
    lsem, xss, xrs, xas, xar, zss, zrs, yds, ydr, yfs, yfr,
    kvs, kvr, hs, hr, rs, rr, als, alr,
):
    z = lax.axis_index("sp")
    y = lax.axis_index("fs")
    t = lax.axis_index("tp")
    x = t // 2
    c = t % 2

    def zz(i):
        return (i + 2 * NZ) % NZ

    def yy(i):
        return (i + 2 * NY) % NY

    def xx(i):
        return (i + 2 * NX) % NX

    dev_z = ({"sp": zz(z + 1)}, {"sp": zz(z - 1)})
    dev_zz = ({"sp": zz(z + 2)}, {"sp": zz(z - 2)})
    dev_y = ({"fs": yy(y + 1)}, {"fs": yy(y - 1)})
    dev_x = ({"tp": xx(x + 1) * 2 + c}, {"tp": xx(x - 1) * 2 + c})
    other = x * 2 + (1 - c)
    dev_c = {"tp": other}
    group = tuple({"tp": (t + i) % 8} for i in range(1, 8))
    dev_far = {"fs": yy(y + 2)}
    peers = dev_z + dev_zz + dev_y + (dev_far,) + group

    def rc(src, dst, ssem, rsem, dev):
        return pltpu.make_async_remote_copy(
            src_ref=src, dst_ref=dst, send_sem=ssem, recv_sem=rsem,
            device_id=dev, device_id_type=MESH,
        )

    own = (
        (tok_ref, xg.at[t]),
        (wk_ref, w0.at[z, y, :, 0:128]),
        (wv_ref, w0.at[z, y, :, 128:256]),
        (wq_ref, w1.at[z, y]),
        (wao_ref, wa.at[t, z, y]),
        (wpost_ref, w2.at[z, y, :, 0:256]),
        (wpre_ref, w2.at[z, y, :, 256:512]),
        (winner_ref, w2.at[z, y, :, 512:768]),
        (wco_ref, w3.at[z, y]),
        (ngain_hbm, ngain_ref),
        (qgain_hbm, qgain_ref),
        (kgain_hbm, kgain_ref),
        (hgain_hbm, hgain_ref),
        (taps_hbm, taps_ref),
        (lam_hbm, lam_ref),
    )
    local = [pltpu.make_async_copy(s, d, lsem.at[i]) for i, (s, d) in enumerate(own)]
    for cp in local:
        cp.start()
    barrier = pltpu.get_barrier_semaphore()
    for dev in peers:
        pl.semaphore_signal(barrier, inc=1, device_id=dev, device_id_type=MESH)

    qb[...] = jnp.zeros_like(qb)
    m_s[...] = jnp.full_like(m_s, -1e30)
    l_s[...] = jnp.zeros_like(l_s)
    acc_s[...] = jnp.zeros_like(acc_s)

    pl.semaphore_wait(barrier, len(peers))

    own_wa = wa.at[t]
    ws = (w0, w1, w2, w3, own_wa)
    zsteps = ((7, 8), (8, 7), (7, 8), (8, 7), (8, 7))

    def z_slab(d, s):
        return zz(z - s) if d == 0 else zz(z + s)

    def z_copy(g, d, s, stride=1):
        ref = ws[g].at[z_slab(d, s - stride), y]
        dev = (dev_z if stride == 1 else dev_zz)[d]
        return rc(ref, ref, zss.at[g, d, s - 1], zrs.at[g, d, s - 1], dev)

    def z_wait(g, d, s):
        ref = ws[g].at[z_slab(d, s), y]
        rc(ref, ref, zss.at[g, d, s - 1], zrs.at[g, d, s - 1], dev_z[d]).wait_recv()

    def z_serve(s):
        for g in (2, 3):
            for d in range(2):
                if s <= zsteps[g][d]:
                    z_wait(g, d, s)
                    if s < zsteps[g][d]:
                        z_copy(g, d, s + 1).start()

    def level(s):
        return (0,) if s == 0 else (15,) if s == 8 else (2 * s - 1, 2 * s)

    def slab_at(k):
        return zz(z + (k + 1) // 2 * (1 - 2 * (k % 2)))

    def y_direct(g, k, d, mine):
        col = y if mine else yy(y - 1) if d == 0 else yy(y + 1)
        ref = ws[g].at[slab_at(k), col]
        return rc(ref, ref, yds.at[g, d, k], ydr.at[g, d, k], dev_y[d])

    def y_half(g, k, d, mine):
        col = yy(y + 2) if not mine else yy(y - 1) if d == 0 else yy(y + 1)
        ref = ws[g].at[slab_at(k), col, pl.ds(16 * d, 16)]
        return rc(ref, ref, yfs.at[g, d, k], yfr.at[g, d, k], dev_y[d])

    def y_send(g, *steps):
        for s in steps:
            for k in level(s):
                for d in range(2):
                    y_direct(g, k, d, True).start()

    def y_relay(g, *steps):
        for s in steps:
            for k in level(s):
                for d in range(2):
                    y_direct(g, k, d, False).wait_recv()
                    y_half(g, k, d, True).start()

    def y_far(g, k, mine):
        ref = ws[g].at[slab_at(k), y if mine else yy(y + 2)]
        return rc(ref, ref, yfs.at[g, 0, k], yfr.at[g, 0, k], dev_far)

    def y_done(g, *steps):
        for s in steps:
            for k in level(s):
                for d in range(2):
                    y_half(g, k, d, False).wait_recv()

    left, right, far = xx(x - 1), xx(x + 1), xx(x + 2)

    def x_gather(buf, lo, hi, ss, sr, start):
        def send(k, slot, dev, piece=None):
            ref = buf.at[slot] if piece is None else buf.at[slot, piece]
            start(rc(ref, ref, ss.at[k], sr.at[k], dev))

        def wait(k, slot, piece=None):
            ref = buf.at[slot] if piece is None else buf.at[slot, piece]
            rc(ref, ref, ss.at[k], sr.at[k], dev_c).wait_recv()

        def begin():
            send(0, t, dev_x[0])
            send(1, t, dev_x[1])
            send(2, t, dev_c)

        def middle():
            wait(0, left * 2 + c)
            send(5, left * 2 + c, dev_x[0], lo)
            wait(1, right * 2 + c)
            send(6, right * 2 + c, dev_x[1], hi)
            send(3, left * 2 + c, dev_c)
            send(4, right * 2 + c, dev_c)

        def late():
            wait(5, far * 2 + c, lo)
            send(7, far * 2 + c, dev_c, lo)
            wait(6, far * 2 + c, hi)
            send(8, far * 2 + c, dev_c, hi)

        def finish():
            wait(2, other)
            wait(3, left * 2 + (1 - c))
            wait(4, right * 2 + (1 - c))
            wait(7, far * 2 + (1 - c), lo)
            wait(8, far * 2 + (1 - c), hi)

        def drain():
            for k, slot, piece in (
                (0, t, None), (1, t, None), (2, t, None),
                (5, left * 2 + c, lo), (6, right * 2 + c, hi),
                (3, left * 2 + c, None), (4, right * 2 + c, None),
                (7, far * 2 + c, lo), (8, far * 2 + c, hi),
            ):
                ref = buf.at[slot] if piece is None else buf.at[slot, piece]
                rc(ref, ref, ss.at[k], sr.at[k], dev_c).wait_send()

        return begin, middle, late, finish, drain

    x_begin, x_service_a, x_service_b, x_finish, x_drain = x_gather(
        xg, pl.ds(0, 256), pl.ds(256, 256), xss, xrs, lambda copy: copy.start()
    )
    a_begin, a_middle, a_late, a_finish, a_drain = x_gather(
        wa, pl.ds(0, 8), pl.ds(8, 8), xas, xar, lambda copy: copy.start()
    )

    for i in (1, 2):
        local[i].wait()
    for stride in (1, 2):
        for d in range(2):
            z_copy(0, d, stride, stride).start()
    local[0].wait()
    x_begin()
    y_send(0, 0)
    local[3].wait()
    for stride in (1, 2):
        for d in range(2):
            z_copy(1, d, stride, stride).start()
    for i in range(4, 9):
        local[i].wait()
    for stride in (1, 2):
        for d in range(2):
            z_copy(4, d, stride, stride).start()
    for g in (2, 3):
        for d in range(2):
            z_copy(g, d, 1).start()
    for i in range(9, len(local)):
        local[i].wait()

    def normalize():
        def tile(i, carry):
            rows = pl.ds(pl.multiple_of(i * 32, 32), 32)
            total = jnp.zeros((32, 256), F32)
            for b in range(8):
                v = xg[b, rows, :].astype(F32)
                total = total + v * v
            r = lax.rsqrt(jnp.sum(total, axis=-1, keepdims=True) * (1.0 / 2048) + EPS)
            for b in range(8):
                v = xg[b, rows, :].astype(F32) * r * ngain_ref[:, b * 256 : (b + 1) * 256]
                nrm[rows, b * 256 : (b + 1) * 256] = v.astype(BF16)
            return carry

        lax.fori_loop(0, 16, tile, 0)

    def z_strides(g, r):
        for s in (2 * r - 1, 2 * r):
            for d in range(2):
                if s <= zsteps[g][d]:
                    z_wait(g, d, s)
                    if s + 2 <= zsteps[g][d]:
                        z_copy(g, d, s + 2, 2).start()

    def z_round(r):
        z_strides(0, r)
        y_send(0, 2 * r - 1, 2 * r)
        if r > 1:
            z_strides(1, r - 1)
        if r > 2:
            z_strides(4, r - 2)

    far_slabs = level(7) + level(8)

    z_round(1)
    y_relay(0, 0)
    y_send(1, 0)
    y_send(2, 0)
    z_serve(1)
    z_round(2)
    x_service_a()
    y_relay(0, 1, 2)
    y_send(1, 1, 2)
    y_send(2, 1)
    z_serve(2)
    z_round(3)
    y_relay(0, 3, 4)
    y_relay(1, 0)
    y_send(1, 3)
    z_serve(3)
    x_service_b()
    z_round(4)
    for k in far_slabs:
        y_far(0, k, True).start()
    y_relay(0, 5, 6)
    y_send(1, 4, 5, 6)
    y_relay(2, 0)
    y_send(4, 0, 1, 2, 3, 4)
    z_serve(4)
    x_finish()
    normalize()
    z_strides(1, 4)
    z_strides(4, 3)
    y_send(1, 7, 8)
    y_send(4, 5, 6)
    y_done(0, *range(7))
    for k in far_slabs:
        y_far(0, k, False).wait_recv()
        for d in range(2):
            y_direct(0, k, d, False).wait_recv()

    def half_norm(v, gain):
        first = lax.broadcasted_iota(jnp.int32, v.shape, 1) < 64
        sq = v * v
        s1 = jnp.sum(jnp.where(first, sq, 0.0), axis=-1, keepdims=True)
        s2 = jnp.sum(jnp.where(first, 0.0, sq), axis=-1, keepdims=True)
        r = jnp.where(
            first, lax.rsqrt(s1 * (1.0 / 64) + EPS), lax.rsqrt(s2 * (1.0 / 64) + EPS)
        )
        return v * r * gain

    kgain = jnp.concatenate([kgain_ref[...]] * 2, axis=1)
    qgain = jnp.concatenate([qgain_ref[...]] * 2, axis=1)

    def kv_tile(i, carry):
        rows = pl.ds(pl.multiple_of(i * 256, 256), 256)
        kv = jnp.dot(nrm[rows, :], w0[...].reshape(2048, 256), preferred_element_type=F32)
        kb[z, rows, :] = half_norm(kv[:, 0:128], kgain).astype(BF16)
        vb[z, :, rows] = kv[:, 128:256].T.astype(BF16)
        return carry

    def q_tile(i, carry):
        rows = pl.ds(pl.multiple_of(i * 128, 128), 128)
        rows2 = pl.ds(pl.multiple_of(i * 128 + 512, 128), 128)
        q = jnp.dot(
            nrm[rows, :], w1[...].reshape(2048, 128), preferred_element_type=F32
        )
        qt = half_norm(q, qgain).T.astype(BF16)
        qb[0:64, rows] = qt[0:64]
        qb[64:128, rows2] = qt[64:128]
        return carry

    lax.fori_loop(0, 2, kv_tile, 0)

    bufs = (kb, vb)

    def kv_copy(d, w, s):
        i = zz(z - (s - 1)) if d == 0 else zz(z + (s - 1))
        ref = bufs[w].at[i]
        return rc(ref, ref, kvs.at[d, w, s - 1], kvr.at[d, w, s - 1], dev_z[d])

    def kv_wait(d, w, s):
        i = zz(z - s) if d == 0 else zz(z + s)
        ref = bufs[w].at[i]
        rc(ref, ref, kvs.at[d, w, s - 1], kvr.at[d, w, s - 1], dev_z[d]).wait_recv()

    factor = LOG2E * 0.125

    for d in range(2):
        kv_copy(d, 0, 1).start()
    z_serve(5)
    for d in range(2):
        kv_copy(d, 1, 1).start()
    y_relay(1, 1, 2, 3, 4)
    y_relay(2, 1)
    y_relay(4, 0, 1)
    z_strides(4, 4)
    y_send(4, 7, 8)
    y_send(2, 2, 3)
    y_relay(1, 5, 6, 7, 8)
    y_relay(4, 2, 3, 4)

    def attend(b):
        cols = [slice(i * 256, i * 256 + 256) for i in range(4)]
        st = [jnp.dot(kb[b], qb[:, cs], preferred_element_type=F32) for cs in cols]
        for i, cs in enumerate(cols):
            m_old = m_s[:, cs]
            m_new = jnp.maximum(m_old, jnp.max(st[i], axis=0, keepdims=True))
            p = jnp.exp2((st[i] - m_new) * factor)
            a = jnp.exp2((m_old - m_new) * factor)
            l_s[:, cs] = l_s[:, cs] * a + jnp.sum(p, axis=0, keepdims=True)
            acc_s[:, cs] = acc_s[:, cs] * a + jnp.dot(
                vb[b], p.astype(BF16), preferred_element_type=F32
            )
            m_s[:, cs] = m_new

    def conv_project(half):
        def tile(j, carry):
            i = 3 * j if half == 0 else 1 + j
            rows = pl.ds(pl.multiple_of(i * 128, 128), 128)
            rows8 = pl.ds(pl.multiple_of(i * 128 + 8, 8), 128)
            r = jnp.dot(nrm[rows, :], w2[...].reshape(2048, 768), preferred_element_type=F32)
            postb[rows, :] = r[:, 0:256].astype(BF16)
            signal = (r[:, 256:512] * r[:, 512:768]).astype(BF16)
            sigb[rows, :] = signal
            sigf[rows8, :] = signal.astype(F32)
            return carry

        lax.fori_loop(0, 2, tile, 0)

    def halo_copy(d):
        src = sigb.at[pl.ds(496, 16)] if d == 0 else sigb.at[pl.ds(0, 16)]
        return rc(src, halo.at[d], hs.at[d], hr.at[d], dev_z[d])

    def conv_filter():
        before = halo[0].astype(F32)[8:16]
        after = halo[1].astype(F32)[0:8]
        sigf[0:8, :] = jnp.where(z > 0, before, 0.0)
        sigf[520:528, :] = jnp.where(z < NZ - 1, after, 0.0)
        taps = taps_ref[:, pl.ds(pl.multiple_of(t * 256, 256), 256)]
        for i in range(4):
            r = i * 128
            filtered = (
                taps[0:1] * sigf[r + 7 : r + 135, :]
                + taps[1:2] * sigf[r + 8 : r + 136, :]
                + taps[2:3] * sigf[r + 9 : r + 137, :]
            )
            conv[r : r + 128, :] = (
                postb[r : r + 128, :].astype(F32) * filtered
            ).astype(BF16)

    up, down = pl.ds(0, 32), pl.ds(32, 32)

    def conv_out(q):
        def tile(j, carry):
            k = 4 * q + 2 * j
            w = jnp.concatenate(
                [w3[slab_at(k + i)].reshape(128, 256) for i in range(2)], axis=0
            )
            r = lax.dot_general(
                conv[...], w, (((1,), (1,)), ((), ())), preferred_element_type=F32
            )
            cols = pl.ds(pl.multiple_of(j * 256, 256), 256)
            part[q, :, :, :, cols] = r.astype(BF16).reshape(NX, 2, 64, 256)
            return carry

        lax.fori_loop(0, 2, tile, 0)

    def sums(q, i):
        p, f = psum.at[q], fin.at[q]
        src, dst, dev = (
            (part.at[q, :, 1 - c], pair_in.at[q], dev_c),
            (p.at[far, up], rel.at[q, 0], dev_x[0]),
            (p.at[far, down], rel.at[q, 1], dev_x[1]),
            (p.at[right, down], f.at[0, down], dev_x[0]),
            (p.at[left, up], f.at[1, up], dev_x[1]),
            (p.at[right, up], f.at[0, up], dev_x[0]),
            (p.at[left, down], f.at[1, down], dev_x[1]),
        )[i]
        return rc(src, dst, rs.at[q, i], rr.at[q, i], dev)

    def sum_pair(q, j):
        psum[q, j] = (part[q, j, c].astype(F32) + pair_in[q, j].astype(F32)).astype(BF16)

    def sum_start(q, *steps):
        y_done(3, *steps)
        conv_out(q)
        sums(q, 0).start()

    def sum_first(q):
        sums(q, 0).wait_recv()
        sum_pair(q, far)
        sums(q, 1).start()
        sums(q, 2).start()
        sum_pair(q, right)
        sum_pair(q, left)
        sums(q, 3).start()
        sums(q, 4).start()

    def sum_second(q):
        sums(q, 1).wait_recv()
        psum[q, right, 0:32] = (
            psum[q, right, 0:32].astype(F32) + rel[q, 0].astype(F32)
        ).astype(BF16)
        sums(q, 5).start()
        sums(q, 2).wait_recv()
        psum[q, left, 32:64] = (
            psum[q, left, 32:64].astype(F32) + rel[q, 1].astype(F32)
        ).astype(BF16)
        sums(q, 6).start()

    def sum_last(q):
        for i in (3, 4, 5, 6):
            sums(q, i).wait_recv()
        total = part[q, x, c].astype(F32) + pair_in[q, x].astype(F32)
        total = total + fin[q, 0].astype(F32) + fin[q, 1].astype(F32)
        for i in range(4):
            col = pl.multiple_of(slab_at(4 * q + i) * 128, 128)
            acc_o[:, pl.ds(col, 128)] = total[:, i * 128 : i * 128 + 128]

    def relay(w, s):
        for d in range(2):
            kv_wait(d, w, s)
            if d == w:
                kv_copy(d, w, s + 1).start()
            else:

                @pl.when(s < 7)
                def _():
                    kv_copy(d, w, s + 1).start()

    def halo_send():
        for d in range(2):
            halo_copy(d).start()

    def conv_finish():
        for d in range(2):
            halo_copy(d).wait_recv()
        conv_filter()

    jobs = {
        (1, 0): lambda: (z_serve(6), y_relay(4, 5, 6), y_send(2, 4)),
        (1, 1): lambda: (y_relay(4, 7, 8), y_relay(2, 2), y_send(2, 5)),
        (2, 0): lambda: (z_serve(7), y_relay(2, 3), y_send(2, 6)),
        (2, 1): lambda: (y_relay(2, 4), y_send(2, 7), y_done(4, *range(9)), a_begin()),
        (3, 0): lambda: (z_serve(8), y_relay(2, 5), y_send(2, 8)),
        (3, 1): lambda: (y_relay(2, 6),),
        (4, 0): lambda: (y_relay(2, 7), y_send(3, 0, 1)),
        (4, 1): lambda: (y_relay(2, 8), y_send(3, 2, 3, 4, 5, 6, 7, 8)),
        (5, 0): lambda: (y_relay(3, 0, 1), y_done(2, *range(9)), conv_project(0), halo_send()),
        (5, 1): lambda: (y_relay(3, 2, 3, 4, 5), conv_project(1), a_middle()),
        (6, 0): lambda: (y_relay(3, 6, 7, 8), conv_finish(), sum_start(0, 0, 1, 2)),
        (6, 1): lambda: (sum_start(1, 3, 4), sum_start(2, 5, 6), sum_first(0)),
        (7, 0): lambda: (sum_start(3, 7, 8), sum_first(1), sum_first(2)),
        (7, 1): lambda: (sum_first(3), a_late(), sum_second(0)),
    }

    def serve(s, w):
        for (at, half), job in jobs.items():
            if half == w:

                @pl.when(s == at)
                def _(job=job):
                    job()

    relay(0, 1)
    jobs[1, 0]()
    relay(1, 1)
    jobs[1, 1]()
    y_done(1, *range(9))
    lax.fori_loop(0, 4, q_tile, 0)
    attend(z)

    def kv_step(s, carry):
        relay(0, s)
        serve(s, 0)
        attend(zz(z - (s - 1)))
        relay(1, s)
        serve(s, 1)
        attend(zz(z + (s - 1)))
        return carry

    lax.fori_loop(2, 8, kv_step, 0)
    attend(zz(z - 7))
    sum_second(1)
    sum_second(2)
    attend(zz(z + 7))
    sum_second(3)
    kv_wait(0, 0, 8)
    kv_wait(1, 1, 8)
    attend(zz(z + 8))

    lane = lax.broadcasted_iota(jnp.int32, (1, 8), 1)
    lam = jnp.sum(jnp.where(lane == t, lam_ref[...], 0.0), axis=1, keepdims=True)
    inv = 1.0 / l_s[...]
    head = acc_s[:, 0:512] * inv[:, 0:512] - lam * (acc_s[:, 512:1024] * inv[:, 512:1024])
    r = lax.rsqrt(jnp.sum(head * head, axis=0, keepdims=True) * (1.0 / 128) + EPS)
    hid[...] = ((head * r).T * hgain_ref[...]).astype(BF16)

    def give(i):
        peer = (t + i) % 8
        rows = pl.ds(pl.multiple_of(peer * 64, 64), 64)
        return rc(hid.at[rows], ah.at[t], als.at[i - 1], alr.at[i - 1], {"tp": peer})

    for i in range(1, 8):
        give(i).start()
    ah[t] = hid[pl.ds(pl.multiple_of(t * 64, 64), 64), :]
    a_finish()
    for q in range(4):
        sum_last(q)
    def out_part(chip, last):
        rows = jnp.concatenate([ah[2 * chip], ah[2 * chip + 1]], axis=1)
        for n in range(8):
            w = jnp.concatenate(
                [wa[2 * chip + i, 2 * n : 2 * n + 2].reshape(256, 128) for i in range(2)], axis=1
            )
            r = lax.dot_general(rows, w, (((1,), (1,)), ((), ())), preferred_element_type=F32)
            cols = slice(n * 256, n * 256 + 256)
            if last:
                out_ref[:, cols] = (acc_o[:, cols] + r).astype(BF16)
            else:
                acc_o[:, cols] = acc_o[:, cols] + r

    def ah_pair(hop):
        for core in range(2):
            source = xx(x + hop) * 2 + core
            slot = (t - source + 8) % 8 - 1
            rc(ah.at[source], ah.at[source], als.at[slot], alr.at[slot], dev_c).wait_recv()

    own_slot = (t - other + 8) % 8 - 1
    rc(ah.at[other], ah.at[other], als.at[own_slot], alr.at[own_slot], dev_c).wait_recv()
    out_part(x, False)
    ah_pair(1)
    out_part(right, False)
    ah_pair(-1)
    out_part(left, False)
    ah_pair(2)
    out_part(far, True)

    for g in range(5):
        for d in range(2):
            for step in range(1, zsteps[g][d] + 1):
                z_copy(g, d, step, 2 if g in (0, 1, 4) and step > 1 else 1).wait_send()

    def y_drain(k, carry):
        for g in range(5):
            for d in range(2):
                y_direct(g, k, d, True).wait_send()
                if g > 0:
                    y_half(g, k, d, True).wait_send()
        return carry

    lax.fori_loop(0, 16, y_drain, 0)

    def y_drain_0(k, carry):
        for d in range(2):
            y_half(0, k, d, True).wait_send()
        return carry

    lax.fori_loop(0, 13, y_drain_0, 0)
    for k in far_slabs:
        y_far(0, k, True).wait_send()
    for w in range(2):
        for d in range(2):
            for s in range(1, 9 if d == w else 8):
                kv_copy(d, w, s).wait_send()
    x_drain()
    a_drain()
    for d in range(2):
        halo_copy(d).wait_send()
    for q in range(4):
        for i in range(7):
            sums(q, i).wait_send()
    for i in range(1, 8):
        give(i).wait_send()


def per_device(
    inputs, norm_gain, query_weight, key_weight, value_weight, query_gain, key_gain,
    mix_lambda, head_gain, post_gate_weight, pre_gate_weight, inner_weight, conv_taps,
    attn_out_weight, conv_out_weight,
):
    hbm = pl.BlockSpec(memory_space=pl.ANY)
    vmem = pl.BlockSpec(memory_space=pltpu.VMEM)
    sem = pltpu.SemaphoreType.DMA
    out = pl.pallas_call(
        body,
        out_shape=jax.ShapeDtypeStruct((64, 2048), BF16),
        in_specs=[hbm] * 15,
        out_specs=vmem,
        scratch_shapes=[
            pltpu.VMEM((1, 2048), F32),
            pltpu.VMEM((1, 64), F32),
            pltpu.VMEM((1, 64), F32),
            pltpu.VMEM((1, 128), F32),
            pltpu.VMEM((3, 2048), F32),
            pltpu.VMEM((1, 8), F32),
            pltpu.VMEM((8, 512, 256), BF16),
            pltpu.VMEM((512, 2048), BF16),
            pltpu.VMEM((NZ, NY, 32, 256), BF16),
            pltpu.VMEM((NZ, NY, 32, 128), BF16),
            pltpu.VMEM((8, NZ, NY, 32, 128), BF16),
            pltpu.VMEM((NZ, NY, 32, 768), BF16),
            pltpu.VMEM((NZ, NY, 32, 256), BF16),
            pltpu.VMEM((NZ, 512, 128), BF16),
            pltpu.VMEM((NZ, 128, 512), BF16),
            pltpu.VMEM((128, 1024), BF16),
            pltpu.VMEM((1, 1024), F32),
            pltpu.VMEM((1, 1024), F32),
            pltpu.VMEM((128, 1024), F32),
            pltpu.VMEM((512, 128), BF16),
            pltpu.VMEM((8, 64, 128), BF16),
            pltpu.VMEM((512, 256), BF16),
            pltpu.VMEM((512, 256), BF16),
            pltpu.VMEM((528, 256), F32),
            pltpu.VMEM((2, 16, 256), BF16),
            pltpu.VMEM((512, 256), BF16),
            pltpu.VMEM((4, NX, 2, 64, 512), BF16),
            pltpu.VMEM((4, NX, 64, 512), BF16),
            pltpu.VMEM((4, NX, 64, 512), BF16),
            pltpu.VMEM((4, 2, 32, 512), BF16),
            pltpu.VMEM((4, 2, 64, 512), BF16),
            pltpu.VMEM((64, 2048), F32),
            sem((15,)),
            sem((9,)),
            sem((9,)),
            sem((9,)),
            sem((9,)),
            sem((5, 2, 8)),
            sem((5, 2, 8)),
            sem((5, 2, 16)),
            sem((5, 2, 16)),
            sem((5, 2, 16)),
            sem((5, 2, 16)),
            sem((2, 2, 8)),
            sem((2, 2, 8)),
            sem((2,)),
            sem((2,)),
            sem((4, 7)),
            sem((4, 7)),
            sem((7,)),
            sem((7,)),
        ],
        compiler_params=pltpu.CompilerParams(
            collective_id=0, has_side_effects=True, vmem_limit_bytes=60 * 1024 * 1024,
        ),
    )(
        inputs[0], query_weight, key_weight, value_weight, post_gate_weight,
        pre_gate_weight, inner_weight, attn_out_weight, conv_out_weight,
        norm_gain.reshape(1, -1),
        query_gain.reshape(1, -1),
        key_gain.reshape(1, -1),
        head_gain.reshape(1, -1),
        conv_taps,
        mix_lambda.reshape(1, -1),
    )
    return out[None]


def solution(mesh):
    rows = P(("sp", "fs"), "tp")
    placed = (
        P("fs", "sp", "tp"), P(), rows, rows, rows, P(), P(), P(), P(),
        rows, rows, rows, P(), rows, rows,
    )
    return jax.shard_map(
        per_device,
        mesh=mesh,
        in_specs=placed,
        out_specs=P("fs", ("sp", "tp"), None),
        check_vma=False,
    )
```
